512 devices in a mesh: sp: 128 (over z, y, core), tp: 4 (over x).
Axes of the slice: x: 4, y: 8, z: 8, core: 2. Of those that a mesh axis runs over, the one named last changes fastest.
Arguments:
- tokens_in: bfloat16 [32768, 2048], P('sp'), may hold values from -6 to 6
- norm_gain: float32 [2048], replicated, may hold values from 0.1 to 1.9
- rec_query_weight: bfloat16 [2048, 1024], P('sp', 'tp'), may hold values from -0.125 to 0.125
- rec_forget_weight: bfloat16 [2048, 1024], P('sp', 'tp'), may hold values from -0.125 to 0.125
- rec_input_weight: bfloat16 [2048, 1024], P('sp', 'tp'), may hold values from -0.125 to 0.125
- att_query_weight: bfloat16 [2048, 1024], P('sp', 'tp'), may hold values from -0.18991481 to 0.18991481
- att_key_weight: bfloat16 [2048, 1024], P('sp', 'tp'), may hold values from -0.18991481 to 0.18991481
- att_value_weight: bfloat16 [2048, 1024], P('sp', 'tp'), may hold values from -0.125 to 0.125
- recurrence_output_weight: bfloat16 [1024, 2048], P('tp'), may hold values from -0.125 to 0.125
- out_att_weight: bfloat16 [1024, 2048], P('tp'), may hold values from -0.125 to 0.125
- floor_gap: float32 [1024], P('tp'), may hold values from 0 to 0.1
- decay_shift: float32 [8, 32768], P('tp', 'sp'), may hold values from -1.5 to 0
- rec_gain: float32 [128], replicated, may hold values from 0.1 to 1.9
- att_gain: float32 [128], replicated, may hold values from 0.1 to 1.9
- lambda_head: float32 [8], P('tp'), may hold values from 0.3 to 0.8
Outputs:
- mixed: bfloat16 [32768, 2048], P('sp')
The draws below stay inside these ranges and needn't reach their ends.
All inputs are finite; a program needn't handle non-finite values.
Results may differ from the reference program's by a relative error of at most 0.015.
Values may be sent and summed in bfloat16 or wider, within the bound.
A program may use at most 128 MiB of HBM per device.

```python
import math
import jax
import jax.numpy as jnp
from jax import lax

D = 2048
REC_HEADS = 8
REC_KEY = 128
REC_VAL = 128
ATT_HEADS = 8
PAIR = 64
ATT_VAL = 128
BLOCK = 64
TOK_DEV = 256
SEQS = 3
SEQ_LEN = 8192
TOKENS = 32768
REC_WIDTH = 1024
ATT_WIDTH = 1024
N_TP = 4


def score_matrix(key, salt):
    normal = jax.random.normal(jax.random.fold_in(key, salt), (D, ATT_HEADS * 2 * PAIR), jnp.float32)
    return jnp.clip(normal, -4.0, 4.0) * (1.32 / math.sqrt(D))


def draw_tokens_in(key, part):
    noise_key = jax.random.fold_in(key, 11)
    return jnp.clip(jax.random.normal(noise_key, (TOKENS, D), jnp.float32), -6.0, 6.0).astype(jnp.bfloat16)


def draw_att_query_weight(key, part):
    matrix = score_matrix(key, 21)
    return matrix.astype(jnp.bfloat16)


def draw_att_key_weight(key, part):
    matrix = score_matrix(key, 22)
    return matrix.astype(jnp.bfloat16)


def draw_floor_gap(key, part):
    fast_head = jax.random.bernoulli(jax.random.fold_in(key, 31), 0.5, (REC_HEADS,))
    fast_channel = jnp.repeat(fast_head, REC_KEY)
    slow_rate = jnp.exp(jax.random.uniform(jax.random.fold_in(key, 32), (REC_HEADS * REC_KEY,), jnp.float32, math.log(0.5), math.log(2.0))) / SEQ_LEN
    fast_rate = jnp.exp(jax.random.uniform(jax.random.fold_in(key, 33), (REC_HEADS * REC_KEY,), jnp.float32, math.log(0.03), math.log(0.1)))
    return jnp.where(fast_channel, fast_rate, slow_rate)


def draw_decay_shift(key, part):
    dev_blocks = TOKENS // TOK_DEV
    rate_key = jax.random.fold_in(key, 41)
    rates = jnp.exp(jax.random.uniform(rate_key, (REC_HEADS, dev_blocks), jnp.float32, math.log(0.2), math.log(0.8)))
    smooth = -jnp.repeat(rates, TOK_DEV, axis=1) / SEQ_LEN
    spots = jax.random.randint(jax.random.fold_in(key, 42), (REC_HEADS, SEQS, 2), 0, SEQ_LEN)
    spots = spots + (jnp.arange(SEQS, dtype=jnp.int32) * SEQ_LEN + SEQ_LEN // 2)[None, :, None]
    drops = jnp.log(jax.random.uniform(jax.random.fold_in(key, 43), (REC_HEADS, SEQS, 2), jnp.float32, 0.5, 0.8))
    hits = jnp.arange(TOKENS, dtype=jnp.int32)[None, None, None, :] == spots[:, :, :, None]
    return smooth + jnp.sum(jnp.where(hits, drops[:, :, :, None], 0.0), axis=(1, 2))


def level_of(key, extent, shards, least, high):
    loudness, own = 1.0, jax.random.fold_in(key, 6)
    for axis_at, parts in shards:
        draws = jnp.exp(jax.random.uniform(jax.random.fold_in(own, axis_at), (parts,), jnp.float32, least / len(shards), high / len(shards)))
        loudness = loudness * jnp.repeat(draws, extent[axis_at] // parts).reshape([-1 if axis == axis_at else 1 for axis in range(len(extent))])
    return loudness


def centred(key, shape, width, reach, split=(), kind=jnp.bfloat16):
    factor_of = level_of(key, shape, split, -0.22, 0.18) if split else 1.0
    result = jax.random.normal(key, shape, jnp.float32) * width * factor_of
    return jnp.minimum(jnp.maximum(result, -reach), reach).astype(kind)


def setup_inputs(seed: int = 0) -> dict:
    key_of = jax.random.split(jax.random.key(seed), 16)
    return {
        "tokens_in": draw_tokens_in(jax.random.fold_in(key_of[15], 71), 0),
        "norm_gain": jnp.clip(1.0 + 0.18 * jax.random.normal(key_of[1], (D,), jnp.float32), 0.1, 1.9),
        "rec_query_weight": centred(key_of[2], (D, REC_HEADS * REC_KEY), D ** -0.5, 0.125, ((0, 128), (1, 4))),
        "rec_forget_weight": centred(key_of[3], (D, REC_HEADS * REC_KEY), D ** -0.5, 0.125, ((0, 128), (1, 4))),
        "rec_input_weight": centred(key_of[4], (D, REC_WIDTH), D ** -0.5, 0.125, ((0, 128), (1, 4))),
        "att_query_weight": draw_att_query_weight(jax.random.fold_in(key_of[15], 71), 0),
        "att_key_weight": draw_att_key_weight(jax.random.fold_in(key_of[15], 71), 0),
        "att_value_weight": centred(key_of[7], (D, ATT_WIDTH), D ** -0.5, 0.125, ((0, 128), (1, 4))),
        "recurrence_output_weight": centred(key_of[8], (REC_WIDTH, D), (REC_WIDTH + ATT_WIDTH) ** -0.5, 0.125, ((0, 4),)),
        "out_att_weight": centred(key_of[9], (ATT_WIDTH, D), (REC_WIDTH + ATT_WIDTH) ** -0.5, 0.125, ((0, 4),)),
        "floor_gap": draw_floor_gap(jax.random.fold_in(key_of[15], 71), 0),
        "decay_shift": draw_decay_shift(jax.random.fold_in(key_of[15], 71), 0),
        "rec_gain": jnp.clip(1.0 + 0.18 * jax.random.normal(key_of[12], (REC_VAL,), jnp.float32), 0.1, 1.9),
        "att_gain": jnp.clip(1.0 + 0.18 * jax.random.normal(key_of[13], (ATT_VAL,), jnp.float32), 0.1, 1.9),
        "lambda_head": jnp.clip(0.3 + 0.5 * jax.random.uniform(key_of[14], (ATT_HEADS,), jnp.float32) ** level_of(key_of[14], (ATT_HEADS,), ((0, 4),), -0.2, 0.2), 0.3, 0.8),
    }


RECUR_EPSILON = 1e-06
ATTEND_EPSILON = 1e-05
ROTARY_BASE = 10000.0
TOP_PRECISION = lax.Precision.HIGHEST

def rms_scale(values, scales, epsilon):
    mean_sq = lax.optimization_barrier(jnp.mean(values * values, axis=-1, keepdims=True))
    return values * lax.rsqrt(mean_sq + epsilon) * scales

def rotary(values, positions):
    half_width = values.shape[-1] // 2
    frequency = 1.0 / ROTARY_BASE ** (jnp.arange(half_width, dtype=jnp.float32) / half_width)
    angles = positions[:, None] * frequency[None, :]
    cosine = jnp.cos(angles)[:, None, :]
    sine_part = jnp.sin(angles)[:, None, :]
    first_half = values[..., :half_width]
    second_half = values[..., half_width:]
    return jnp.concatenate([first_half * cosine - second_half * sine_part, second_half * cosine + first_half * sine_part], axis=-1)

def recur_blocks(queries, gate_key_rows, inputs, log_decay, keep_flags, carry_in):
    head_count = queries.shape[0]
    length = queries.shape[1]
    block_count = length // BLOCK

    def split_blocks(array):
        return array.reshape(head_count, block_count, BLOCK, array.shape[-1]).transpose(1, 0, 2, 3)
    causal = jnp.tril(jnp.ones((BLOCK, BLOCK), dtype=bool))

    def advance(carried, bundle):
        q_block, k_block, v_block, g_block, keep_now = bundle
        carried = carried * keep_now
        cum_log = jnp.cumsum(g_block, axis=1)
        q_decayed = q_block * jnp.exp(cum_log)
        k_growth = k_block * jnp.exp(-cum_log)
        from_past = jnp.einsum('hcd,hde->hce', q_decayed, carried, precision=TOP_PRECISION)
        scores = jnp.einsum('htd,hsd->hts', q_decayed, k_growth, precision=TOP_PRECISION)
        scores = jnp.where(causal[None], scores, 0.0)
        within = jnp.einsum('hts,hse->hte', scores, v_block, precision=TOP_PRECISION)
        end_log = cum_log[:, -1:, :]
        k_to_end = k_block * jnp.exp(end_log - cum_log)
        fresh = jnp.exp(end_log[:, 0, :])[:, :, None] * carried + jnp.einsum('hsd,hse->hde', k_to_end, v_block, precision=TOP_PRECISION)
        return (fresh, from_past + within)
    final_state, outputs = lax.scan(advance, carry_in, (split_blocks(queries), split_blocks(gate_key_rows), split_blocks(inputs), split_blocks(log_decay), keep_flags))
    return (outputs.transpose(1, 0, 2, 3).reshape(head_count, length, inputs.shape[-1]), final_state)

def attend_sequence(queries, seq_keys, seq_values, segment, lambda_head):
    seq_length = queries.shape[0]
    query_rows = math.gcd(seq_length, 512)
    score_scale = queries.shape[-1] ** (-0.5)
    key_index = jnp.arange(seq_length, dtype=jnp.int32)
    keys_wide = seq_keys.astype(jnp.float32)
    values_wide = seq_values.astype(jnp.float32)

    def one_block(bundle):
        first_row, q_block, q_segment = bundle
        scores = jnp.einsum('qhcd,khcd->hcqk', q_block.astype(jnp.float32), keys_wide) * score_scale
        causal = (first_row + jnp.arange(query_rows, dtype=jnp.int32))[:, None] >= key_index[None, :]
        causal = causal & (q_segment[:, None] == segment[None, :])
        scores = jnp.where(causal, scores, -jnp.inf)
        best_score = lax.optimization_barrier(jnp.max(scores, axis=-1))
        expo_vals = jnp.exp(scores - best_score[..., None])
        totals = lax.optimization_barrier(jnp.sum(expo_vals, axis=-1))
        rounded = lax.optimization_barrier(expo_vals.astype(jnp.bfloat16)).astype(jnp.float32)
        weighted = jnp.einsum('hcqk,khe->hcqe', rounded, values_wide)
        mixed_raw = weighted[:, 0] / totals[:, 0, :, None] - lambda_head[:, None, None] * weighted[:, 1] / totals[:, 1, :, None]
        return mixed_raw.transpose(1, 0, 2)
    block_total = seq_length // query_rows
    starts = jnp.arange(block_total, dtype=jnp.int32) * query_rows
    blocks = queries.reshape(block_total, query_rows, queries.shape[1], 2, queries.shape[-1])
    return lax.map(one_block, (starts, blocks, segment.reshape(block_total, query_rows))).reshape(seq_length, queries.shape[1], seq_values.shape[-1])

def reference(tokens_in, norm_gain, rec_query_weight, rec_forget_weight, rec_input_weight, att_query_weight, att_key_weight, att_value_weight, recurrence_output_weight, out_att_weight, floor_gap, decay_shift, rec_gain, att_gain, lambda_head):
    normed = rms_scale(tokens_in.astype(jnp.float32), norm_gain, RECUR_EPSILON).astype(jnp.bfloat16)

    def project(weight):
        return jnp.dot(normed, weight, preferred_element_type=jnp.float32)
    half_seq = SEQ_LEN // 2
    token_index = jnp.arange(TOKENS, dtype=jnp.int32)
    seq_start = jnp.maximum(0, (token_index + half_seq) // SEQ_LEN * SEQ_LEN - half_seq).astype(jnp.int32)
    rec_query = project(rec_query_weight).astype(jnp.bfloat16)
    rec_forget = project(rec_forget_weight).astype(jnp.bfloat16)
    rec_input = project(rec_input_weight).astype(jnp.bfloat16)
    positions = (token_index - seq_start).astype(jnp.float32)
    att_query = rotary(project(att_query_weight).reshape(TOKENS, ATT_HEADS * 2, PAIR), positions).astype(jnp.bfloat16)
    att_key = rotary(project(att_key_weight).reshape(TOKENS, ATT_HEADS * 2, PAIR), positions).astype(jnp.bfloat16)
    att_value = project(att_value_weight).astype(jnp.bfloat16)
    gate_key = floor_gap[None, :] * jax.nn.sigmoid(-rec_forget.astype(jnp.float32))
    log_decay = jnp.log1p(-gate_key).reshape(TOKENS, REC_HEADS, REC_KEY) + decay_shift.T[:, :, None]

    def by_head(array):
        return array.reshape(TOKENS, REC_HEADS, -1).transpose(1, 0, 2)
    block_starts = jnp.arange(TOKENS // BLOCK, dtype=jnp.int32) * BLOCK
    keep_flags = jnp.where(seq_start[block_starts] == block_starts, 0.0, 1.0).astype(jnp.float32)
    rec_raw = recur_blocks(by_head(rec_query.astype(jnp.float32)), by_head(gate_key), by_head(rec_input.astype(jnp.float32)), log_decay.transpose(1, 0, 2), keep_flags, jnp.zeros((REC_HEADS, REC_KEY, REC_VAL), jnp.float32))[0]
    rec_raw = rec_raw.transpose(1, 0, 2)
    rec_mix = rms_scale(rec_raw, rec_gain, RECUR_EPSILON).astype(jnp.bfloat16).reshape(TOKENS, REC_WIDTH)

    def attend_one(bundle):
        return attend_sequence(bundle[0], bundle[1], bundle[2], bundle[3], lambda_head)
    group_count = TOKENS // SEQ_LEN
    seq_shape = (group_count, SEQ_LEN, ATT_HEADS, 2, PAIR)

    def rolled(array):
        return jnp.roll(array, -half_seq, axis=0)
    att_raw = lax.map(attend_one, (rolled(att_query).reshape(seq_shape), rolled(att_key).reshape(seq_shape), rolled(att_value).reshape(group_count, SEQ_LEN, ATT_HEADS, ATT_VAL), rolled(seq_start).reshape(group_count, SEQ_LEN)))
    att_raw = jnp.roll(att_raw.reshape(TOKENS, ATT_HEADS, ATT_VAL), half_seq, axis=0)
    att_mix = rms_scale(att_raw, att_gain, ATTEND_EPSILON).astype(jnp.bfloat16).reshape(TOKENS, ATT_WIDTH)
    rec_rows = REC_WIDTH // N_TP
    att_rows = ATT_WIDTH // N_TP
    summed = jnp.zeros((TOKENS, D), jnp.float32)
    for group in range(N_TP):
        partial_value = jnp.dot(rec_mix[:, group * rec_rows:(group + 1) * rec_rows], recurrence_output_weight[group * rec_rows:(group + 1) * rec_rows], preferred_element_type=jnp.float32)
        partial_value = partial_value + jnp.dot(att_mix[:, group * att_rows:(group + 1) * att_rows], out_att_weight[group * att_rows:(group + 1) * att_rows], preferred_element_type=jnp.float32)
        summed = summed + lax.optimization_barrier(partial_value.astype(jnp.bfloat16)).astype(jnp.float32)
    return summed.astype(jnp.bfloat16)
```

```python
import functools

import jax
import jax.numpy as jnp
from jax import lax
from jax.experimental import pallas as pl
from jax.experimental.pallas import tpu as pltpu
from jax.sharding import Mesh
from jax.sharding import PartitionSpec as P

HEAD = 128
PAIR = 64
BLOCK = 64
SP = ("sp_0", "sp_1", "sp_2")
NZ, NY, NX = 8, 8, 4
HALF = NY // 2
TOK = 256
QUART = TOK // NX
ST_ROWS = 144
RECUR_EPSILON = 1e-06
ATTEND_EPSILON = 1e-05
ROTARY_BASE = 10000.0
SCORE_LOG2 = PAIR ** (-0.5) * 1.4426950408889634
F32, BF16 = jnp.float32, jnp.bfloat16
MESH_ID = pl.DeviceIdType.MESH
NT = (((1,), (1,)), ((), ()))


def remote(src, dst, send, recv, where):
    return pltpu.make_async_remote_copy(
        src_ref=src, dst_ref=dst, send_sem=send, recv_sem=recv, device_id=where, device_id_type=MESH_ID
    )


def greet(places):
    barrier = pltpu.get_barrier_semaphore()
    for place in places:
        pl.semaphore_signal(barrier, inc=1, device_id=place, device_id_type=MESH_ID)
    pl.semaphore_wait(barrier, len(places))


def where_am_i():
    return (lax.axis_index("sp_0"), lax.axis_index("sp_1"), lax.axis_index("sp_2"), lax.axis_index("tp"))


def partner_row(z):
    return jnp.where(z % 2 == 1, (z + 1) % NZ, (z + NZ - 1) % NZ)


class Ring:
    def __init__(self, y, c, first, piece, sems):
        self.y, self.c, self.first, self.piece = y, c, first, piece
        self.sr, self.rr, self.sl, self.rl, self.sp, self.rp = sems
        self.right = {"sp_1": (y + 1) % NY}
        self.left = {"sp_1": (y + NY - 1) % NY}
        self.other = {"sp_2": 1 - c}

    def source(self, offset, h):
        if offset == 0:
            return self.first(h)
        return self.piece((self.y + offset + NY) % NY, self.c, h)

    def to_right(self, k, h):
        origin = (self.y - (k - 1) + NY) % NY
        i = 2 * (k - 1) + h
        return remote(
            self.source(1 - k, h), self.piece(origin, self.c, h), self.sr.at[i], self.rr.at[i], self.right
        )

    def to_left(self, k, h):
        origin = (self.y + (k - 1)) % NY
        i = 2 * (k - 1) + h
        return remote(
            self.source(k - 1, h), self.piece(origin, self.c, h), self.sl.at[i], self.rl.at[i], self.left
        )

    def to_other(self, offset, h):
        i = 2 * (offset % NY) + h
        origin = (self.y + offset + NY) % NY
        return remote(
            self.source(offset, h), self.piece(origin, self.c, h), self.sp.at[i], self.rp.at[i], self.other
        )

    def from_side(self, offset, h, sems, i):
        ref = self.piece((self.y + offset + NY) % NY, self.c, h)
        return remote(ref, ref, self.sr.at[0], sems.at[i], self.right)

    def goes_right(self, k, h):
        return k < HALF or (k == HALF and h == 0)

    def goes_left(self, k, h):
        return k < HALF or (k == HALF and h == 1)

    def begin(self):
        for h in range(2):
            self.to_right(1, h).start()
            self.to_left(1, h).start()
        for h in range(2):
            self.to_other(0, h).start()

    def step(self, k, h):
        if self.goes_right(k, h):
            self.from_side(-k, h, self.rr, 2 * (k - 1) + h).wait_recv()
            if self.goes_right(k + 1, h):
                self.to_right(k + 1, h).start()
            self.to_other(-k, h).start()
        if self.goes_left(k, h):
            self.from_side(k, h, self.rl, 2 * (k - 1) + h).wait_recv()
            if self.goes_left(k + 1, h):
                self.to_left(k + 1, h).start()
            self.to_other(k, h).start()

    def wait_other(self, offset, h):
        ref = self.piece((self.y + offset + NY) % NY, 1 - self.c, h)
        remote(ref, ref, self.sp.at[0], self.rp.at[2 * (offset % NY) + h], self.other).wait_recv()

    def finish(self):
        for k in range(1, HALF + 1):
            for h in range(2):
                if self.goes_right(k, h):
                    self.to_right(k, h).wait_send()
                if self.goes_left(k, h):
                    self.to_left(k, h).wait_send()
        for offset in range(NY):
            for h in range(2):
                self.to_other(offset, h).wait_send()


def ring_sems():
    return [
        pltpu.SemaphoreType.DMA((2 * HALF,)),
        pltpu.SemaphoreType.DMA((2 * HALF,)),
        pltpu.SemaphoreType.DMA((2 * HALF,)),
        pltpu.SemaphoreType.DMA((2 * HALF,)),
        pltpu.SemaphoreType.DMA((2 * NY,)),
        pltpu.SemaphoreType.DMA((2 * NY,)),
    ]


def project_kernel(
    x_ref, w_ref, ds_ref, gain_ref, cos_ref, sin_ref,
    rec_ref, q_ref, kv_ref, dso_ref,
    xp, xn, wbuf, dsp,
    t1s, t1r, t2s, t2r, dss, dsr, w1s, w1r, *sems,
):
    z, y, c, x = where_am_i()
    zp = partner_row(z)
    row = (z + 1) % 2
    right, left = (x + 1) % NX, (x + NX - 1) % NX
    greet(
        [{"sp_0": (z + d) % NZ} for d in range(1, NZ)]
        + [{"tp": right}, {"tp": left}]
        + [{"sp_1": (y + 1) % NY}, {"sp_1": (y + NY - 1) % NY}, {"sp_2": 1 - c}]
    )
    across = remote(x_ref.at[x], xp.at[x], t1s.at[0], t1r.at[0], {"sp_0": zp})
    spread = []
    for d in (1, 7, 2, 6, 3, 5, 4):
        there = (z + d) % NZ
        spread.append(
            remote(
                w_ref.at[(there + 1) % 2], wbuf.at[z, y, c], w1s.at[d - 1], w1r.at[d - 1], {"sp_0": there}
            )
        )
    for copy in spread:
        copy.start()
    across.start()
    shifts = remote(ds_ref, dsp, dss.at[0], dsr.at[0], {"sp_0": zp})
    shifts.start()
    wbuf[z, y, c] = w_ref[row]

    def normed(values):
        values = values.astype(F32)
        mean_sq = jnp.mean(values * values, axis=-1, keepdims=True)
        return (values * lax.rsqrt(mean_sq + RECUR_EPSILON) * gain_ref[...]).astype(BF16)

    for d in range(1, NZ):
        ref = wbuf.at[(z + NZ - d) % NZ, y, c]
        remote(ref, ref, w1s.at[d - 1], w1r.at[d - 1], {"sp_0": zp}).wait_recv()
    piece = lambda yo, stream, h: wbuf.at[pl.ds(h * (NZ // 2), NZ // 2), yo, stream]
    ring = Ring(y, c, lambda h: piece(y, c, h), piece, sems)
    ring.begin()
    across.wait_recv()
    to_right = remote(xp.at[x], xp.at[x], t2s.at[0], t2r.at[0], {"tp": right})
    to_left = remote(xp.at[x], xp.at[x], t2s.at[1], t2r.at[1], {"tp": left})
    to_right.start()
    to_left.start()
    for i in range(NX):
        xn[row, pl.ds(i * QUART, QUART)] = normed(x_ref[i])
    ring.step(1, 0)
    ring.step(1, 1)
    half = QUART // 2
    mine_l, mine_r = xp.at[left], xp.at[right]
    remote(mine_l, mine_l, t2s.at[0], t2r.at[0], {"tp": right}).wait_recv()
    far_l = xp.at[left, pl.ds(0, half)]
    on_right = remote(far_l, far_l, t2s.at[2], t2r.at[2], {"tp": right})
    on_right.start()
    remote(mine_r, mine_r, t2s.at[1], t2r.at[1], {"tp": left}).wait_recv()
    far_r = xp.at[right, pl.ds(half, half)]
    on_left = remote(far_r, far_r, t2s.at[3], t2r.at[3], {"tp": left})
    on_left.start()
    for k in range(2, HALF + 1):
        for h in range(2):
            ring.step(k, h)
    opposite = (x + 2) % NX
    got_a = xp.at[opposite, pl.ds(0, half)]
    got_b = xp.at[opposite, pl.ds(half, half)]
    remote(got_a, got_a, t2s.at[2], t2r.at[2], {"tp": right}).wait_recv()
    remote(got_b, got_b, t2s.at[3], t2r.at[3], {"tp": left}).wait_recv()
    for i in range(NX):
        xn[1 - row, pl.ds(i * QUART, QUART)] = normed(xp[i])
    shifts.wait_recv()
    dso_ref[pl.ds(row, 1)] = ds_ref[pl.ds(row, 1)]
    dso_ref[pl.ds(1 - row, 1)] = dsp[pl.ds(row, 1)]
    for offset in range(NY):
        for h in range(2):
            ring.wait_other(offset, h)

    lane = lax.broadcasted_iota(jnp.int32, (TOK, HEAD), 1)
    first = (lane % PAIR) < (PAIR // 2)

    def turned(values, kind):
        swapped = jnp.where(
            first, pltpu.roll(values, HEAD - PAIR // 2, 1), pltpu.roll(values, PAIR // 2, 1)
        )
        return (values * cos_ref[kind] + swapped * sin_ref[kind]).astype(BF16)

    for part in range(3):
        weight = wbuf[:, :, :, :, pl.ds(part * 256, 256)].reshape(NZ * NY * 2 * 16, 256)
        for kind in range(2):
            out = jnp.dot(xn[kind], weight, preferred_element_type=F32)
            one, two = out[:, :HEAD], out[:, HEAD:]
            if part == 0:
                rec_ref[0, kind] = one.astype(BF16)
                rec_ref[1, kind] = two.astype(BF16)
            elif part == 1:
                rec_ref[2, kind] = one.astype(BF16)
                kv_ref[kind, :, pl.ds(HEAD, HEAD)] = two.astype(BF16)
            else:
                q_ref[kind] = turned(one, kind)
                kv_ref[kind, :, pl.ds(0, HEAD)] = turned(two, kind)
    ring.finish()
    for copy in spread:
        copy.wait_send()
    for copy in (across, shifts, to_right, to_left, on_right, on_left):
        copy.wait_send()


def mix_kernel(
    rec_ref, q_ref, kv_ref, ds_ref, fg_ref, lam_ref, rgain_ref, again_ref,
    mix_ref,
    kvbuf, stbuf, q2, m_s, l_s, acc, local, qdec, *sems,
):
    z, y, c, x = where_am_i()
    row = (z + 1) % 2
    linked = jnp.logical_and(z != 0, z != NZ - 1)
    greet([{"sp_1": (y + 1) % NY}, {"sp_1": (y + NY - 1) % NY}, {"sp_2": 1 - c}])
    kv_ring = Ring(
        y, c, lambda h: kv_ref.at[h], lambda yo, stream, h: kvbuf.at[yo, h, stream], sems[:6]
    )
    st_ring = Ring(
        y, c, lambda h: stbuf.at[y, c, h], lambda yo, stream, h: stbuf.at[yo, stream, h], sems[6:]
    )
    kv_ring.begin()
    kvbuf[y, 0, c] = kv_ref[0]
    kvbuf[y, 1, c] = kv_ref[1]

    causal = lax.broadcasted_iota(jnp.int32, (BLOCK, BLOCK), 0) >= lax.broadcasted_iota(
        jnp.int32, (BLOCK, BLOCK), 1
    )
    tril = jnp.where(causal, 1.0, 0.0).astype(F32)
    gap = fg_ref[pl.ds(row, 1)]

    def segment(kind):
        shift = jnp.broadcast_to(ds_ref[pl.ds(kind, 1)], (HEAD, TOK)).T
        state = jnp.zeros((HEAD, HEAD), F32)
        total = jnp.zeros((1, HEAD), F32)
        for b in range(TOK // BLOCK):
            rows = pl.ds(b * BLOCK, BLOCK)
            forget = rec_ref[1, kind, rows].astype(F32)
            query = rec_ref[0, kind, rows].astype(F32)
            value = rec_ref[2, kind, rows]
            gate = gap * (1.0 / (1.0 + jnp.exp(forget)))
            decay = jnp.log1p(-gate) + shift[b * BLOCK : (b + 1) * BLOCK]
            cum = jnp.dot(tril, decay, precision=lax.Precision.HIGHEST, preferred_element_type=F32)
            end = cum[BLOCK - 1 :, :]
            q_dec = query * jnp.exp(cum)
            qdec[kind, rows] = (q_dec * jnp.exp(total)).astype(BF16)
            q_dec = q_dec.astype(BF16)
            k_grow = (gate * jnp.exp(-cum)).astype(BF16)
            scores = lax.dot_general(q_dec, k_grow, NT, preferred_element_type=F32)
            scores = jnp.where(causal, scores, 0.0).astype(BF16)
            out = jnp.dot(scores, value, preferred_element_type=F32)
            if b > 0:
                out = out + lax.dot_general(q_dec, state.astype(BF16), NT, preferred_element_type=F32)
            local[kind, rows] = out
            k_end = (gate * jnp.exp(end - cum)).astype(BF16)
            fresh = jnp.dot(value.astype(F32).T.astype(BF16), k_end, preferred_element_type=F32)
            state = state * jnp.exp(end) + fresh
            total = total + end
        stbuf[y, c, kind, pl.ds(0, HEAD)] = state.astype(BF16)
        high = total.astype(BF16)
        rest = total - high.astype(F32)
        middle = rest.astype(BF16)
        low = (rest - middle.astype(F32)).astype(BF16)
        index = lax.broadcasted_iota(jnp.int32, (ST_ROWS - HEAD, HEAD), 0)
        stack = jnp.where(
            index == 0, high.astype(F32), jnp.where(index == 1, middle.astype(F32), low.astype(F32))
        )
        stbuf[y, c, kind, pl.ds(HEAD, ST_ROWS - HEAD)] = stack.astype(BF16)

    segment(0)
    segment(1)
    st_ring.begin()

    lane = lax.broadcasted_iota(jnp.int32, (TOK, HEAD), 1)
    for kind in range(2):
        q_all = q_ref[kind].astype(F32)
        q2[kind, pl.ds(0, TOK)] = jnp.where(lane < PAIR, q_all, 0.0).astype(BF16)
        q2[kind, pl.ds(TOK, TOK)] = jnp.where(lane >= PAIR, q_all, 0.0).astype(BF16)

    def keys_values(yo, kind):
        both = kvbuf[yo, kind].reshape(2 * TOK, 2 * HEAD)
        return both[:, :HEAD], both[:, HEAD:]

    for h in range(2):
        kv_ring.wait_other(0, h)

    def own(kind, carry):
        keys, values = keys_values(y, kind)
        for part in range(2):
            rows = pl.ds(part * TOK, TOK)
            scores = lax.dot_general(q2[kind, rows], keys, NT, preferred_element_type=F32)
            seen = lax.broadcasted_iota(jnp.int32, (TOK, 2 * TOK), 1) <= (
                lax.broadcasted_iota(jnp.int32, (TOK, 2 * TOK), 0) + c * TOK
            )
            scores = jnp.where(seen, scores, -jnp.inf)
            best = jnp.max(scores, axis=-1, keepdims=True)
            expo = jnp.exp2((scores - best) * SCORE_LOG2)
            m_s[kind, rows] = jnp.broadcast_to(best, (TOK, HEAD))
            l_s[kind, rows] = jnp.broadcast_to(jnp.sum(expo, axis=-1, keepdims=True), (TOK, HEAD))
            acc[kind, rows] = jnp.dot(expo.astype(BF16), values, preferred_element_type=F32)
        return carry

    lax.fori_loop(0, 2, own, 0)

    def absorb(yo, q_kind, kv_kind):
        keys, values = keys_values(yo, kv_kind)
        for part in range(2):
            rows = pl.ds(part * TOK, TOK)
            scores = lax.dot_general(q2[q_kind, rows], keys, NT, preferred_element_type=F32)
            old = m_s[q_kind, rows]
            best = jnp.maximum(old, jnp.max(scores, axis=-1, keepdims=True))
            scale = jnp.exp2((old - best) * SCORE_LOG2)
            expo = jnp.exp2((scores - best[:, :1]) * SCORE_LOG2)
            m_s[q_kind, rows] = best
            l_s[q_kind, rows] = l_s[q_kind, rows] * scale + jnp.sum(expo, axis=-1, keepdims=True)
            acc[q_kind, rows] = acc[q_kind, rows] * scale + jnp.dot(
                expo.astype(BF16), values, preferred_element_type=F32
            )

    def process(offsets):
        for offset in offsets:
            for h in range(2):
                if offset:
                    kv_ring.wait_other(offset, h)

        def unit(i, carry):
            which = i // 3
            kind_at = i % 3
            offset = jnp.where(which == 0, offsets[0], offsets[-1])
            yo = (y + offset + NY) % NY
            q_kind = jnp.where(kind_at == 0, 0, 1)
            kv_kind = jnp.where(kind_at == 2, 1, 0)
            wanted = jnp.where(kind_at == 1, linked.astype(jnp.int32), (yo < y).astype(jnp.int32))

            @pl.when(wanted == 1)
            def _():
                absorb(yo, q_kind, kv_kind)

            return carry

        lax.fori_loop(0, 3 * len(offsets), unit, 0)

    for k in range(1, HALF + 1):
        for h in range(2):
            kv_ring.step(k, h)
        if k == 1:
            process((0,))
        else:
            process((1 - k, k - 1))
        for h in range(2):
            st_ring.step(k, h)
    process((HALF,))
    for offset in range(NY):
        for h in range(2):
            st_ring.wait_other(offset, h)

    me = 2 * y + c

    def pass_on(kind, s, state):
        yo, stream = s // 2, s % 2
        tail = stbuf[yo, stream, kind, pl.ds(HEAD, ST_ROWS - HEAD)].astype(F32)
        total = tail[0:1] + tail[1:2] + tail[2:3]
        return state * jnp.exp(total) + stbuf[yo, stream, kind, pl.ds(0, HEAD)].astype(F32)

    nothing = jnp.zeros((HEAD, HEAD), F32)
    into_low = lax.fori_loop(0, me, functools.partial(pass_on, 0), nothing)
    all_low = lax.fori_loop(me, 2 * NY, functools.partial(pass_on, 0), into_low)
    all_low = all_low * jnp.where(linked, 1.0, 0.0)
    into_high = lax.fori_loop(0, me, functools.partial(pass_on, 1), all_low)
    lam = lam_ref[row]
    for kind in range(2):
        state = (into_low if kind == 0 else into_high).astype(BF16)
        raw = local[kind] + lax.dot_general(qdec[kind], state, NT, preferred_element_type=F32)
        mean_sq = jnp.mean(raw * raw, axis=-1, keepdims=True)
        mix_ref[kind, :, pl.ds(0, HEAD)] = (
            raw * lax.rsqrt(mean_sq + RECUR_EPSILON) * rgain_ref[...]
        ).astype(BF16)
        raw = acc[kind, pl.ds(0, TOK)] / l_s[kind, pl.ds(0, TOK)] - lam * (
            acc[kind, pl.ds(TOK, TOK)] / l_s[kind, pl.ds(TOK, TOK)]
        )
        mean_sq = jnp.mean(raw * raw, axis=-1, keepdims=True)
        mix_ref[kind, :, pl.ds(HEAD, HEAD)] = (
            raw * lax.rsqrt(mean_sq + ATTEND_EPSILON) * again_ref[...]
        ).astype(BF16)
    kv_ring.finish()
    st_ring.finish()


def output_kernel(
    mix_ref, wr_ref, wa_ref, out_ref,
    other, part, relay, got,
    ms, mr, s_sem, r_sem, g_send, g_recv,
):
    z, y, c, x = where_am_i()
    row = (z + 1) % 2
    right, left, far = (x + 1) % NX, (x + NX - 1) % NX, (x + 2) % NX
    to_r, to_l = {"tp": right}, {"tp": left}
    zp = {"sp_0": partner_row(z)}
    greet([to_r, to_l, zp])
    swap = remote(mix_ref.at[1 - row], other, ms.at[0], mr.at[0], zp)
    swap.start()
    swap.wait_recv()
    rows_own = pl.ds(row * HEAD, HEAD)
    rows_other = pl.ds((1 - row) * HEAD, HEAD)
    own = mix_ref[row]
    theirs = other[...]
    width = 512
    for j in range(2048 // width):
        cols = pl.ds(j * width, width)
        total = jnp.dot(own[:, :HEAD], wr_ref[rows_own, cols], preferred_element_type=F32)
        total += jnp.dot(own[:, HEAD:], wa_ref[rows_own, cols], preferred_element_type=F32)
        total += jnp.dot(theirs[:, :HEAD], wr_ref[rows_other, cols], preferred_element_type=F32)
        total += jnp.dot(theirs[:, HEAD:], wa_ref[rows_other, cols], preferred_element_type=F32)
        total = total.astype(BF16)
        for i in range(NX):
            part[i, :, cols] = total[i * QUART : (i + 1) * QUART]
    half = QUART // 2
    top, low = pl.ds(0, half), pl.ds(half, half)
    sends = [
        remote(part.at[far, top], relay.at[0], s_sem.at[0], r_sem.at[0], to_r),
        remote(part.at[far, low], relay.at[1], s_sem.at[1], r_sem.at[1], to_l),
        remote(part.at[right], got.at[0], s_sem.at[2], r_sem.at[2], to_r),
        remote(part.at[left], got.at[1], s_sem.at[3], r_sem.at[3], to_l),
    ]
    for copy in sends:
        copy.start()
    sends[0].wait_recv()
    on_r = remote(relay.at[0], got.at[2, top], s_sem.at[4], r_sem.at[4], to_r)
    on_r.start()
    sends[1].wait_recv()
    on_l = remote(relay.at[1], got.at[2, low], s_sem.at[5], r_sem.at[5], to_l)
    on_l.start()
    sends[2].wait_recv()
    sends[3].wait_recv()
    on_r.wait_recv()
    on_l.wait_recv()
    summed = part[x].astype(F32) + got[0].astype(F32) + got[1].astype(F32) + got[2].astype(F32)
    out_ref[x] = summed.astype(BF16)
    g_r = remote(out_ref.at[x], out_ref.at[x], g_send.at[0], g_recv.at[0], to_r)
    g_l = remote(out_ref.at[x], out_ref.at[x], g_send.at[1], g_recv.at[1], to_l)
    g_r.start()
    g_l.start()
    from_l, from_r = out_ref.at[left], out_ref.at[right]
    remote(from_l, from_l, g_send.at[0], g_recv.at[0], to_r).wait_recv()
    pass_r = out_ref.at[left, top]
    g_rr = remote(pass_r, pass_r, g_send.at[2], g_recv.at[2], to_r)
    g_rr.start()
    remote(from_r, from_r, g_send.at[1], g_recv.at[1], to_l).wait_recv()
    pass_l = out_ref.at[right, low]
    g_ll = remote(pass_l, pass_l, g_send.at[3], g_recv.at[3], to_l)
    g_ll.start()
    far_a, far_b = out_ref.at[far, top], out_ref.at[far, low]
    remote(far_a, far_a, g_send.at[2], g_recv.at[2], to_r).wait_recv()
    remote(far_b, far_b, g_send.at[3], g_recv.at[3], to_l).wait_recv()
    for copy in sends + [swap, on_r, on_l, g_r, g_l, g_rr, g_ll]:
        copy.wait_send()


VM = pl.BlockSpec(memory_space=pltpu.VMEM)
DMA = pltpu.SemaphoreType.DMA


def call(kernel, name, number, shapes, specs, scratch, args):
    return pl.pallas_call(
        kernel,
        name=name,
        out_shape=shapes,
        in_specs=specs,
        out_specs=jax.tree.map(lambda _: VM, shapes),
        scratch_shapes=scratch,
        compiler_params=pltpu.CompilerParams(
            collective_id=number, has_side_effects=True, vmem_limit_bytes=60 * 1024 * 1024
        ),
    )(*args)


def per_device(
    tokens_in, norm_gain, rec_query_weight, rec_forget_weight, rec_input_weight, att_query_weight,
    att_key_weight, att_value_weight, recurrence_output_weight, out_att_weight, floor_gap,
    decay_shift, rec_gain, att_gain, lambda_head,
):
    z, y, c, x = where_am_i()
    weights = jnp.stack(
        [
            w.reshape(16, 2, HEAD)
            for w in (
                rec_query_weight, rec_forget_weight, rec_input_weight,
                att_value_weight, att_query_weight, att_key_weight,
            )
        ],
        axis=2,
    )
    weights = weights.transpose(1, 0, 2, 3).reshape(2, 16, 6 * HEAD)
    linked = jnp.logical_and(z != 0, z != NZ - 1)
    start = (2 * y + c) * TOK + jnp.arange(TOK, dtype=jnp.int32)
    positions = jnp.stack([start, start + jnp.where(linked, 2 * NY * TOK, 0)]).astype(F32)
    width = PAIR // 2
    frequency = 1.0 / ROTARY_BASE ** (jnp.arange(width, dtype=F32) / width)
    angles = positions[:, :, None] * frequency
    cosine, sine = jnp.cos(angles), jnp.sin(angles)
    cosine = jnp.concatenate([cosine] * 4, axis=-1)
    sine = jnp.concatenate([-sine, sine] * 2, axis=-1)
    d_model = tokens_in.shape[1]
    rec, query, kv, shifts = call(
        project_kernel,
        "project",
        0,
        [
            jax.ShapeDtypeStruct((3, 2, TOK, HEAD), BF16),
            jax.ShapeDtypeStruct((2, TOK, HEAD), BF16),
            jax.ShapeDtypeStruct((2, TOK, 2 * HEAD), BF16),
            jax.ShapeDtypeStruct((2, TOK), F32),
        ],
        [VM] * 6,
        [
            pltpu.VMEM((NX, QUART, d_model), BF16),
            pltpu.VMEM((2, TOK, d_model), BF16),
            pltpu.VMEM((NZ, NY, 2, 16, 6 * HEAD), BF16),
            pltpu.VMEM((2, TOK), F32),
            DMA((1,)), DMA((1,)), DMA((4,)), DMA((4,)), DMA((1,)), DMA((1,)), DMA((NZ - 1,)), DMA((NZ - 1,)),
            *ring_sems(),
        ],
        (tokens_in.reshape(NX, QUART, d_model), weights, decay_shift, norm_gain[None], cosine, sine),
    )
    mix = call(
        mix_kernel,
        "mix",
        1,
        jax.ShapeDtypeStruct((2, TOK, 2 * HEAD), BF16),
        [VM] * 5 + [pl.BlockSpec(memory_space=pltpu.SMEM)] + [VM] * 2,
        [
            pltpu.VMEM((NY, 2, 2, TOK, 2 * HEAD), BF16),
            pltpu.VMEM((NY, 2, 2, ST_ROWS, HEAD), BF16),
            pltpu.VMEM((2, 2 * TOK, HEAD), BF16),
            pltpu.VMEM((2, 2 * TOK, HEAD), F32),
            pltpu.VMEM((2, 2 * TOK, HEAD), F32),
            pltpu.VMEM((2, 2 * TOK, HEAD), F32),
            pltpu.VMEM((2, TOK, HEAD), F32),
            pltpu.VMEM((2, TOK, HEAD), BF16),
            *ring_sems(),
            *ring_sems(),
        ],
        (
            rec, query, kv, shifts, floor_gap.reshape(2, HEAD), lambda_head, rec_gain[None], att_gain[None],
        ),
    )
    out = call(
        output_kernel,
        "output",
        2,
        jax.ShapeDtypeStruct((NX, QUART, d_model), BF16),
        [VM] * 3,
        [
            pltpu.VMEM((TOK, 2 * HEAD), BF16),
            pltpu.VMEM((NX, QUART, d_model), BF16),
            pltpu.VMEM((2, QUART // 2, d_model), BF16),
            pltpu.VMEM((3, QUART, d_model), BF16),
            DMA((1,)), DMA((1,)), DMA((6,)), DMA((6,)), DMA((4,)), DMA((4,)),
        ],
        (mix, recurrence_output_weight, out_att_weight),
    )
    return out.reshape(TOK, d_model)


def solution(mesh):
    split = Mesh(mesh.devices.reshape(NZ, NY, 2, NX), ("sp_0", "sp_1", "sp_2", "tp"))
    placed = (
        P(SP, None), P(), P(SP, "tp"), P(SP, "tp"), P(SP, "tp"), P(SP, "tp"), P(SP, "tp"), P(SP, "tp"),
        P("tp", None), P("tp", None), P("tp"), P("tp", SP), P(), P(), P("tp"),
    )
    return jax.shard_map(
        per_device, mesh=split, in_specs=placed, out_specs=P(SP, None), check_vma=False
    )
```

```python
import functools

import jax
import jax.numpy as jnp
import numpy as np
from jax import lax
from jax.experimental import pallas as pl
from jax.experimental.pallas import tpu as pltpu
from jax.sharding import Mesh
from jax.sharding import PartitionSpec as P

HEAD = 128
PAIR = 64
BLOCK = 64
SP = ("sp_0", "sp_1", "sp_2")
NZ, NY, NX = 8, 8, 4
HALF = NY // 2
TOK = 256
QUART = TOK // NX
ST_ROWS = 144
RECUR_EPSILON = 1e-06
ATTEND_EPSILON = 1e-05
ROTARY_BASE = 10000.0
SCORE_LOG2 = PAIR ** (-0.5) * 1.4426950408889634
F32, BF16 = jnp.float32, jnp.bfloat16
DMA = pltpu.SemaphoreType.DMA
VM = pl.BlockSpec(memory_space=pltpu.VMEM)
HBM = pl.BlockSpec(memory_space=pltpu.HBM)
OUT_HALF = 1024
VMEM_LIMIT = 60 * 1024 * 1024
REL = (0, 1, 7, 2, 6, 3, 5, 4)
POS = tuple(REL.index(d) for d in range(NZ))
MESH_ID = pl.DeviceIdType.MESH
NT = (((1,), (1,)), ((), ()))


def remote(src, dst, send, recv, where):
    return pltpu.make_async_remote_copy(
        src_ref=src, dst_ref=dst, send_sem=send, recv_sem=recv, device_id=where, device_id_type=MESH_ID
    )


def greet(places):
    barrier = pltpu.get_barrier_semaphore()
    for place in places:
        pl.semaphore_signal(barrier, inc=1, device_id=place, device_id_type=MESH_ID)
    pl.semaphore_wait(barrier, len(places))


def where_am_i():
    return (lax.axis_index("sp_0"), lax.axis_index("sp_1"), lax.axis_index("sp_2"), lax.axis_index("tp"))


def partner_row(z):
    return jnp.where(z % 2 == 1, (z + 1) % NZ, (z + NZ - 1) % NZ)


class Ring:
    def __init__(self, y, c, parts, piece, sems):
        self.y, self.c, self.parts, self.piece = y, c, parts, piece
        self.sr, self.rr, self.sl, self.rl, self.sp, self.rp = sems
        self.right = {"sp_1": (y + 1) % NY}
        self.left = {"sp_1": (y + NY - 1) % NY}
        self.other = {"sp_2": 1 - c}

    def at(self, offset, i):
        return self.piece((self.y + offset + NY) % NY, self.c, i)

    def index(self, k, i):
        return self.parts * (k - 1) + i

    def to_right(self, k, i):
        ref, n = self.at(1 - k, i), self.index(k, i)
        return remote(ref, ref, self.sr.at[n], self.rr.at[n], self.right)

    def to_left(self, k, i):
        ref, n = self.at(k - 1, i), self.index(k, i)
        return remote(ref, ref, self.sl.at[n], self.rl.at[n], self.left)

    def to_other(self, offset, i):
        ref, n = self.at(offset, i), self.parts * (offset % NY) + i
        return remote(ref, ref, self.sp.at[n], self.rp.at[n], self.other)

    def goes_right(self, k, i):
        return k < HALF or (k == HALF and i < self.parts // 2)

    def goes_left(self, k, i):
        return k < HALF or (k == HALF and i >= self.parts // 2)

    def begin(self, i):
        self.to_right(1, i).start()
        self.to_left(1, i).start()
        self.to_other(0, i).start()

    def step(self, k, i):
        n = self.index(k, i)
        if self.goes_right(k, i):
            ref = self.at(-k, i)
            remote(ref, ref, self.sr.at[n], self.rr.at[n], self.right).wait_recv()
            if self.goes_right(k + 1, i):
                self.to_right(k + 1, i).start()
            self.to_other(-k, i).start()
        if self.goes_left(k, i):
            ref = self.at(k, i)
            remote(ref, ref, self.sl.at[n], self.rl.at[n], self.left).wait_recv()
            if self.goes_left(k + 1, i):
                self.to_left(k + 1, i).start()
            self.to_other(k, i).start()

    def wait_other(self, offset):
        for i in range(self.parts):
            ref = self.piece((self.y + offset + NY) % NY, 1 - self.c, i)
            n = self.parts * (offset % NY) + i
            remote(ref, ref, self.sp.at[n], self.rp.at[n], self.other).wait_recv()

    def finish(self):
        for i in range(self.parts):
            for k in range(1, HALF + 1):
                if self.goes_right(k, i):
                    self.to_right(k, i).wait_send()
                if self.goes_left(k, i):
                    self.to_left(k, i).wait_send()
            for offset in range(NY):
                self.to_other(offset, i).wait_send()


def ring_sems(parts):
    return [DMA((parts * HALF,))] * 4 + [DMA((parts * NY,))] * 2


def layer_kernel(
    x_ref, wq_ref, wf_ref, wi_ref, wv_ref, waq_ref, wak_ref, wr_ref, wa_ref,
    ds_hbm, gain_hbm, freq_hbm, fg_hbm, rgain_hbm, again_hbm, lam_ref,
    out_ref,
    ds_ref, gain_ref, freq_ref, fg_ref, rgain_ref, again_ref,
    xloc, xp, xn, wloc, wbuf, dsp, dso, wobuf,
    rec, kvbuf, stbuf, q2, m_s, l_s, acc, local, qdec, mixs, mb,
    load, t1s, t1r, t2s, t2r, dss, dsr, w1s, w1r, wos, wor, wops, wopr, as_, ar, gs, gr,
    *sems,
):
    z, y, c, x = where_am_i()
    zp = partner_row(z)
    row = (z + 1) % 2
    linked = jnp.logical_and(z != 0, z != NZ - 1)
    right, left, far = (x + 1) % NX, (x + NX - 1) % NX, (x + 2) % NX
    to_r, to_l, core = {"tp": right}, {"tp": left}, {"sp_2": 1 - c}
    half = QUART // 2
    halves = (pl.ds(0, half), pl.ds(half, half))

    loads = []

    def bring(src, dst):
        copy = pltpu.make_async_copy(src, dst, load.at[len(loads)])
        copy.start()
        loads.append(copy)
        return copy

    mine = pl.ds(pl.multiple_of(row * HEAD, HEAD), HEAD)
    yours = pl.ds(pl.multiple_of((1 - row) * HEAD, HEAD), HEAD)
    weight_refs = (wq_ref, wf_ref, wi_ref, wv_ref, waq_ref, wak_ref)
    own_w = [
        bring(ref.at[:, mine], wbuf.at[0, y, c, :, pl.ds(p * HEAD, HEAD)])
        for p, ref in enumerate(weight_refs)
    ]
    other_w = [
        bring(ref.at[:, yours], wloc.at[:, pl.ds(p * HEAD, HEAD)]) for p, ref in enumerate(weight_refs)
    ]
    quarter = bring(x_ref.at[x], xloc.at[x])
    rest_x = [bring(x_ref.at[(x + d) % NX], xloc.at[(x + d) % NX]) for d in range(1, NX)]
    own_wo = [
        bring(ref.at[:, pl.ds(h * OUT_HALF, OUT_HALF)], wobuf.at[x, h, pl.ds(r * 2 * HEAD, 2 * HEAD)])
        for h in range(2)
        for r, ref in enumerate((wr_ref, wa_ref))
    ]

    small = [
        bring(src, dst)
        for src, dst in (
            (ds_hbm, ds_ref), (gain_hbm, gain_ref), (freq_hbm, freq_ref), (fg_hbm, fg_ref),
            (rgain_hbm, rgain_ref), (again_hbm, again_ref),
        )
    ]
    greet(
        [{"sp_0": (z + d) % NZ} for d in range(1, NZ)]
        + [{"tp": (x + d) % NX} for d in range(1, NX)]
        + [{"sp_0": zp, "tp": (x + d) % NX} for d in range(1, NX)]
        + [{"sp_1": (y + 1) % NY}, {"sp_1": (y + NY - 1) % NY}, core]
    )

    def to_row(d):
        src = wbuf.at[0, y, c] if d % 2 == 0 else wloc
        at = POS[(NZ - d) % NZ]
        return remote(
            src, wbuf.at[at, y, c], w1s.at[at - 1], w1r.at[at - 1], {"sp_0": (z + d) % NZ}
        )

    def row_came(at):
        ref = wbuf.at[at, y, c]
        remote(ref, ref, w1s.at[at - 1], w1r.at[at - 1], core).wait_recv()

    spread = {d: to_row(d) for d in range(1, NZ)}
    across = [
        remote(xloc.at[x, rows], xp.at[x, rows], t1s.at[i], t1r.at[i], {"sp_0": zp})
        for i, rows in enumerate(halves)
    ]
    shifts = remote(ds_ref, dsp, dss.at[0], dsr.at[0], {"sp_0": zp})
    for copy in other_w:
        copy.wait()
    spread[1].start()
    spread[7].start()
    quarter.wait()
    across[0].start()
    across[1].start()
    for copy in own_w:
        copy.wait()
    for d in (2, 6, 3, 5, 4):
        spread[d].start()
    for copy in small:
        copy.wait()
    shifts.start()

    for copy in own_wo:
        copy.wait()

    def wo_at(group, i):
        return wobuf.at[group, c, pl.ds(i * HEAD, HEAD)]

    wo_right = [remote(wo_at(x, i), wo_at(x, i), wos.at[i], wor.at[i], to_r) for i in range(4)]
    wo_left = [remote(wo_at(x, i), wo_at(x, i), wos.at[4 + i], wor.at[4 + i], to_l) for i in range(4)]
    wo_on_right = [
        remote(wo_at(left, i), wo_at(left, i), wos.at[8 + i], wor.at[8 + i], to_r) for i in (0, 1)
    ]
    wo_on_left = [
        remote(wo_at(right, i), wo_at(right, i), wos.at[8 + i], wor.at[8 + i], to_l) for i in (2, 3)
    ]
    wo_push = {
        (g, i): remote(
            wo_at((x + g) % NX, i),
            wo_at((x + g) % NX, i),
            wops.at[4 * (g - 1) + i],
            wopr.at[4 * (g - 1) + i],
            core,
        )
        for g in (1, 2, 3)
        for i in range(4)
    }

    def wo_came(group_offset, i, slot):
        ref = wo_at((x + group_offset) % NX, i)
        remote(ref, ref, wos.at[slot], wor.at[slot], to_r).wait_recv()
        wo_push[(group_offset, i)].start()

    wo_right[0].start()
    wo_left[2].start()

    w_ring = Ring(
        y, c, 4, lambda yo, stream, i: wbuf.at[pl.ds(2 * i, 2), yo, stream], sems[0:6]
    )

    def normed(source, kind, i):
        values = source[i].astype(F32)
        mean_sq = jnp.mean(values * values, axis=-1, keepdims=True)
        scale = lax.rsqrt(mean_sq + RECUR_EPSILON)
        for p in range(NZ):
            cols = pl.ds(pl.multiple_of(((z + REL[p]) % NZ) * 256, 256), 256)
            value = source[i, :, cols].astype(F32) * scale * gain_ref[:, cols]
            xn[kind, pl.ds(pl.multiple_of(i * QUART, QUART), QUART), pl.ds(p * 256, 256)] = value.astype(BF16)

    t2_right = [remote(xp.at[x, r], xp.at[x, r], t2s.at[i], t2r.at[i], to_r) for i, r in enumerate(halves)]
    t2_left = [remote(xp.at[x, r], xp.at[x, r], t2s.at[2 + i], t2r.at[2 + i], to_l) for i, r in enumerate(halves)]
    t2_on_right = remote(xp.at[left, halves[0]], xp.at[left, halves[0]], t2s.at[4], t2r.at[4], to_r)
    t2_on_left = remote(xp.at[right, halves[1]], xp.at[right, halves[1]], t2s.at[5], t2r.at[5], to_l)

    def t2_came(group, i, slot):
        ref = xp.at[group, halves[i]]
        remote(ref, ref, t2s.at[slot], t2r.at[slot], to_r).wait_recv()

    row_came(1)
    w_ring.begin(0)
    row_came(2)
    row_came(3)
    w_ring.begin(1)
    for i in range(2):
        across[i].wait_recv()
        t2_right[i].start()
        t2_left[i].start()
        row_came(4 + 2 * i)
        row_came(5 + 2 * i)
        w_ring.begin(2 + i)
    for copy in rest_x:
        copy.wait()
    for i in range(NX):
        w_ring.step(1, i)
        normed(xloc, row, i)
    t2_came(left, 0, 0)
    t2_on_right.start()
    t2_came(right, 1, 3)
    t2_on_left.start()
    for i in (1, 2, 3):
        wo_right[i].start()
    for i in (3, 0, 1):
        wo_left[i].start()
    normed(xp, 1 - row, x)
    t2_came(left, 1, 1)
    t2_came(right, 0, 2)
    for i in range(4):
        w_ring.step(2, i)
        if i == 1:
            normed(xp, 1 - row, left)
        elif i == 3:
            normed(xp, 1 - row, right)
    for i in range(4):
        w_ring.step(3, i)
    t2_came(far, 0, 4)
    t2_came(far, 1, 5)
    normed(xp, 1 - row, far)
    wo_came(3, 0, 0)
    wo_on_right[0].start()
    wo_came(1, 2, 6)
    wo_on_left[0].start()

    lane = lax.broadcasted_iota(jnp.int32, (TOK, HEAD), 1)
    first = (lane % PAIR) < (PAIR // 2)
    place = (2 * y + c) * TOK + lax.broadcasted_iota(jnp.int32, (TOK, HEAD), 0)
    tables = []
    for kind in range(2):
        at = place if kind == 0 else place + jnp.where(linked, 2 * NY * TOK, 0)
        angle = at.astype(F32) * freq_ref[...]
        sine = jnp.sin(angle)
        tables.append((jnp.cos(angle), jnp.where(first, -sine, sine)))
        m_s[kind, pl.ds(0, TOK)] = tables[kind][0]
        l_s[kind, pl.ds(0, TOK)] = tables[kind][1]

    def turned(values, kind):
        swapped = jnp.where(
            first, pltpu.roll(values, HEAD - PAIR // 2, 1), pltpu.roll(values, PAIR // 2, 1)
        )
        return values * m_s[kind, pl.ds(0, TOK)] + swapped * l_s[kind, pl.ds(0, TOK)]

    shifts.wait_recv()
    dso[pl.ds(row, 1)] = ds_ref[pl.ds(row, 1)]
    dso[pl.ds(1 - row, 1)] = dsp[pl.ds(row, 1)]
    for i in range(4):
        w_ring.step(4, i)
    for offset in range(NY):
        w_ring.wait_other(offset)

    def projected(part, kind):
        weight = wbuf[:, :, :, :, pl.ds(part * 256, 256)].reshape(NZ * NY * 2 * 16, 256)
        out = jnp.dot(xn[kind], weight, preferred_element_type=F32)
        return out[:, :HEAD], out[:, HEAD:]

    half_rows = TOK // 2
    kv_ring = Ring(
        y,
        c,
        4,
        lambda yo, stream, i: kvbuf.at[yo, i // 2, stream, pl.ds((i % 2) * half_rows, half_rows)],
        sems[6:12],
    )
    st_ring = Ring(y, c, 2, lambda yo, stream, i: stbuf.at[yo, stream, i], sems[12:18])
    for kind in range(2):
        one, two = projected(2, kind)
        kvbuf[y, kind, c, :, pl.ds(0, HEAD)] = turned(two, kind).astype(BF16)
        query = turned(one, kind)
        q2[kind, pl.ds(0, TOK)] = jnp.where(lane < PAIR, query, 0.0).astype(BF16)
        q2[kind, pl.ds(TOK, TOK)] = jnp.where(lane >= PAIR, query, 0.0).astype(BF16)
        one, two = projected(1, kind)
        kvbuf[y, kind, c, :, pl.ds(HEAD, HEAD)] = two.astype(BF16)
        rec[2, kind] = one.astype(BF16)
    kv_ring.begin(0)
    kv_ring.begin(1)
    for kind in range(2):
        one, two = projected(0, kind)
        rec[0, kind] = one.astype(BF16)
        rec[1, kind] = two.astype(BF16)
        if kind == 0:
            kv_ring.begin(2)
            kv_ring.begin(3)

    causal = lax.broadcasted_iota(jnp.int32, (BLOCK, BLOCK), 0) >= lax.broadcasted_iota(
        jnp.int32, (BLOCK, BLOCK), 1
    )
    tril = jnp.where(causal, 1.0, 0.0).astype(F32)
    gap = fg_ref[pl.ds(row, 1)]

    def segment(kind):
        shift = jnp.broadcast_to(dso[pl.ds(kind, 1)], (HEAD, TOK)).T
        state = jnp.zeros((HEAD, HEAD), F32)
        total = jnp.zeros((1, HEAD), F32)
        for b in range(TOK // BLOCK):
            rows = pl.ds(b * BLOCK, BLOCK)
            forget = rec[1, kind, rows].astype(F32)
            query = rec[0, kind, rows].astype(F32)
            value = rec[2, kind, rows]
            gate = gap * (1.0 / (1.0 + jnp.exp(forget)))
            decay = jnp.log1p(-gate) + shift[b * BLOCK : (b + 1) * BLOCK]
            cum = jnp.dot(tril, decay, precision=lax.Precision.HIGHEST, preferred_element_type=F32)
            end = cum[BLOCK - 1 :, :]
            q_dec = query * jnp.exp(cum)
            qdec[kind, rows] = (q_dec * jnp.exp(total)).astype(BF16)
            q_dec = q_dec.astype(BF16)
            k_grow = (gate * jnp.exp(-cum)).astype(BF16)
            scores = lax.dot_general(q_dec, k_grow, NT, preferred_element_type=F32)
            scores = jnp.where(causal, scores, 0.0).astype(BF16)
            out = jnp.dot(scores, value, preferred_element_type=F32)
            if b > 0:
                out = out + lax.dot_general(q_dec, state.astype(BF16), NT, preferred_element_type=F32)
            local[kind, rows] = out
            k_end = (gate * jnp.exp(end - cum)).astype(BF16)
            fresh = jnp.dot(value.astype(F32).T.astype(BF16), k_end, preferred_element_type=F32)
            state = state * jnp.exp(end) + fresh
            total = total + end
        stbuf[y, c, kind, pl.ds(0, HEAD)] = state.astype(BF16)
        high = total.astype(BF16)
        rest = total - high.astype(F32)
        middle = rest.astype(BF16)
        low = (rest - middle.astype(F32)).astype(BF16)
        index = lax.broadcasted_iota(jnp.int32, (ST_ROWS - HEAD, HEAD), 0)
        stack = jnp.where(
            index == 0, high.astype(F32), jnp.where(index == 1, middle.astype(F32), low.astype(F32))
        )
        stbuf[y, c, kind, pl.ds(HEAD, ST_ROWS - HEAD)] = stack.astype(BF16)

    segment(0)
    kv_ring.step(1, 0)
    kv_ring.step(1, 1)
    segment(1)
    kv_ring.step(1, 2)
    kv_ring.step(1, 3)
    st_ring.begin(0)
    st_ring.begin(1)

    def keys_values(yo, kind):
        both = kvbuf[yo, kind].reshape(2 * TOK, 2 * HEAD)
        return both[:, :HEAD], both[:, HEAD:]

    kv_ring.wait_other(0)

    def own(kind, carry):
        keys, values = keys_values(y, kind)
        for part in range(2):
            rows = pl.ds(part * TOK, TOK)
            scores = lax.dot_general(q2[kind, rows], keys, NT, preferred_element_type=F32)
            seen = lax.broadcasted_iota(jnp.int32, (TOK, 2 * TOK), 1) <= (
                lax.broadcasted_iota(jnp.int32, (TOK, 2 * TOK), 0) + c * TOK
            )
            scores = jnp.where(seen, scores, -jnp.inf)
            best = jnp.max(scores, axis=-1, keepdims=True)
            expo = jnp.exp2((scores - best) * SCORE_LOG2)
            m_s[kind, rows] = jnp.broadcast_to(best, (TOK, HEAD))
            l_s[kind, rows] = jnp.broadcast_to(jnp.sum(expo, axis=-1, keepdims=True), (TOK, HEAD))
            acc[kind, rows] = jnp.dot(expo.astype(BF16), values, preferred_element_type=F32)
        return carry

    lax.fori_loop(0, 2, own, 0)

    def absorb(yo, q_kind, kv_kind):
        keys, values = keys_values(yo, kv_kind)
        for part in range(2):
            rows = pl.ds(part * TOK, TOK)
            scores = lax.dot_general(q2[q_kind, rows], keys, NT, preferred_element_type=F32)
            old = m_s[q_kind, rows]
            best = jnp.maximum(old, jnp.max(scores, axis=-1, keepdims=True))
            scale = jnp.exp2((old - best) * SCORE_LOG2)
            expo = jnp.exp2((scores - best[:, :1]) * SCORE_LOG2)
            m_s[q_kind, rows] = best
            l_s[q_kind, rows] = l_s[q_kind, rows] * scale + jnp.sum(expo, axis=-1, keepdims=True)
            acc[q_kind, rows] = acc[q_kind, rows] * scale + jnp.dot(
                expo.astype(BF16), values, preferred_element_type=F32
            )

    def process(offset):
        if offset:
            kv_ring.wait_other(offset)
        yo = (y + offset + NY) % NY

        def unit(kind_at, carry):
            q_kind = jnp.where(kind_at == 0, 0, 1)
            kv_kind = jnp.where(kind_at == 2, 1, 0)
            wanted = jnp.where(kind_at == 1, linked.astype(jnp.int32), (yo < y).astype(jnp.int32))

            @pl.when(wanted == 1)
            def _():
                absorb(yo, q_kind, kv_kind)

            return carry

        lax.fori_loop(0, 3, unit, 0)

    process(0)
    for k in range(2, HALF + 1):
        kv_ring.step(k, 0)
        kv_ring.step(k, 1)
        process(1 - k)
        kv_ring.step(k, 2)
        kv_ring.step(k, 3)
        st_ring.step(k - 1, 0)
        st_ring.step(k - 1, 1)
        if k == 3:
            wo_came(3, 1, 1)
            wo_on_right[1].start()
            wo_came(1, 3, 7)
            wo_on_left[1].start()
        process(k - 1)
    st_ring.step(HALF, 0)
    st_ring.step(HALF, 1)
    process(HALF)
    for offset in range(NY):
        st_ring.wait_other(offset)

    me = 2 * y + c

    def pass_on(kind, s, state):
        yo, stream = s // 2, s % 2
        tail = stbuf[yo, stream, kind, pl.ds(HEAD, ST_ROWS - HEAD)].astype(F32)
        total = tail[0:1] + tail[1:2] + tail[2:3]
        return state * jnp.exp(total) + stbuf[yo, stream, kind, pl.ds(0, HEAD)].astype(F32)

    nothing = jnp.zeros((HEAD, HEAD), F32)
    into_low = lax.fori_loop(0, me, functools.partial(pass_on, 0), nothing)
    all_low = lax.fori_loop(me, 2 * NY, functools.partial(pass_on, 0), into_low)
    all_low = all_low * jnp.where(linked, 1.0, 0.0)
    into_high = lax.fori_loop(0, me, functools.partial(pass_on, 1), all_low)
    lam = lam_ref[row]

    def mix_to(same, d):
        kind = row if same else 1 - row
        there = (x + d) % NX
        n = d if same else NX + d
        where = {"tp": there} if same else {"sp_0": zp, "tp": there}
        return remote(mixs.at[kind, there], mb.at[x, row], as_.at[n], ar.at[n], where)

    for kind in range(2):
        state = (into_low if kind == 0 else into_high).astype(BF16)
        raw = local[kind] + lax.dot_general(qdec[kind], state, NT, preferred_element_type=F32)
        mean_sq = jnp.mean(raw * raw, axis=-1, keepdims=True)
        rec_mix = (raw * lax.rsqrt(mean_sq + RECUR_EPSILON) * rgain_ref[...]).astype(BF16)
        raw = acc[kind, pl.ds(0, TOK)] / l_s[kind, pl.ds(0, TOK)] - lam * (
            acc[kind, pl.ds(TOK, TOK)] / l_s[kind, pl.ds(TOK, TOK)]
        )
        mean_sq = jnp.mean(raw * raw, axis=-1, keepdims=True)
        att_mix = (raw * lax.rsqrt(mean_sq + ATTEND_EPSILON) * again_ref[...]).astype(BF16)
        for i in range(NX):
            mixs[kind, i, :, pl.ds(0, HEAD)] = rec_mix[i * QUART : (i + 1) * QUART]
            mixs[kind, i, :, pl.ds(HEAD, HEAD)] = att_mix[i * QUART : (i + 1) * QUART]

    mix_sends = [mix_to(False, d) for d in (2, 1, 3, 0)] + [mix_to(True, d) for d in (2, 1, 3)]
    for copy in mix_sends:
        copy.start()
    mb[x, row] = mixs[row, x]

    for i in (1, 2, 3):
        if i != 1:
            wo_came(3, i, i)
    for i in (0, 1):
        wo_came(1, i, 4 + i)
    for i in range(4):
        wo_came(2, i, 8 + i)
    for g in (1, 2, 3):
        for i in range(4):
            ref = wobuf.at[(x + g) % NX, 1 - c, pl.ds(i * HEAD, HEAD)]
            remote(ref, ref, wops.at[4 * (g - 1) + i], wopr.at[4 * (g - 1) + i], core).wait_recv()

    for d in range(NX):
        for same in (True, False):
            if same and d == 0:
                continue
            n = d if same else NX + d
            ref = mb.at[(x + NX - d) % NX, row if same else 1 - row]
            remote(ref, ref, as_.at[n], ar.at[n], core).wait_recv()

    width = OUT_HALF // 2
    groups = [
        jnp.concatenate([mb[g, h][:, p * HEAD : (p + 1) * HEAD] for p in range(2) for h in range(2)], axis=1)
        for g in range(NX)
    ]
    gathers = []
    for j in range(4):
        total = jnp.zeros((QUART, width), F32)
        for g in range(NX):
            weight = wobuf[g, j // 2, :, pl.ds((j % 2) * width, width)]
            total += jnp.dot(groups[g], weight, preferred_element_type=F32).astype(BF16).astype(F32)
        cols = pl.ds(j * width, width)
        out_ref[x, :, cols] = total.astype(BF16)
        ref = out_ref.at[x, :, cols]
        gathers.append(remote(ref, ref, gs.at[4 * j], gr.at[4 * j], to_r))
        gathers.append(remote(ref, ref, gs.at[4 * j + 1], gr.at[4 * j + 1], to_l))
        gathers[-2].start()
        gathers[-1].start()
    for j in range(4):
        cols = pl.ds(j * width, width)
        ref = out_ref.at[left, :, cols]
        remote(ref, ref, gs.at[4 * j], gr.at[4 * j], to_r).wait_recv()
        ref = out_ref.at[left, halves[0], cols]
        gathers.append(remote(ref, ref, gs.at[4 * j + 2], gr.at[4 * j + 2], to_r))
        gathers[-1].start()
        ref = out_ref.at[right, :, cols]
        remote(ref, ref, gs.at[4 * j + 1], gr.at[4 * j + 1], to_l).wait_recv()
        ref = out_ref.at[right, halves[1], cols]
        gathers.append(remote(ref, ref, gs.at[4 * j + 3], gr.at[4 * j + 3], to_l))
        gathers[-1].start()
    for j in range(4):
        cols = pl.ds(j * width, width)
        for i in range(2):
            ref = out_ref.at[far, halves[i], cols]
            remote(ref, ref, gs.at[4 * j + 2 + i], gr.at[4 * j + 2 + i], to_r).wait_recv()
    w_ring.finish()
    kv_ring.finish()
    st_ring.finish()
    sent = list(spread.values()) + across + [shifts] + t2_right + t2_left + [t2_on_right, t2_on_left]
    sent += wo_right + wo_left + wo_on_right + wo_on_left + list(wo_push.values()) + mix_sends + gathers
    for copy in sent:
        copy.wait_send()


def per_device(
    tokens_in, norm_gain, rec_query_weight, rec_forget_weight, rec_input_weight, att_query_weight,
    att_key_weight, att_value_weight, recurrence_output_weight, out_att_weight, floor_gap,
    decay_shift, rec_gain, att_gain, lambda_head,
):
    width = PAIR // 2
    steps = np.arange(width, dtype=np.float32) / np.float32(width)
    frequency = np.float32(1.0) / np.float32(ROTARY_BASE) ** steps
    frequency = np.concatenate([frequency] * 4)[None].astype(np.float32)
    d_model = tokens_in.shape[1]
    out = pl.pallas_call(
        layer_kernel,
        name="layer",
        out_shape=jax.ShapeDtypeStruct((NX, QUART, d_model), BF16),
        in_specs=[HBM] * 15 + [pl.BlockSpec(memory_space=pltpu.SMEM)],
        out_specs=VM,
        scratch_shapes=[
            pltpu.VMEM((2, TOK), F32),
            pltpu.VMEM((1, d_model), F32),
            pltpu.VMEM((1, HEAD), F32),
            pltpu.VMEM((2, HEAD), F32),
            pltpu.VMEM((1, HEAD), F32),
            pltpu.VMEM((1, HEAD), F32),
            pltpu.VMEM((NX, QUART, d_model), BF16),
            pltpu.VMEM((NX, QUART, d_model), BF16),
            pltpu.VMEM((2, TOK, d_model), BF16),
            pltpu.VMEM((16, 6 * HEAD), BF16),
            pltpu.VMEM((NZ, NY, 2, 16, 6 * HEAD), BF16),
            pltpu.VMEM((2, TOK), F32),
            pltpu.VMEM((2, TOK), F32),
            pltpu.VMEM((NX, 2, 4 * HEAD, OUT_HALF), BF16),
            pltpu.VMEM((3, 2, TOK, HEAD), BF16),
            pltpu.VMEM((NY, 2, 2, TOK, 2 * HEAD), BF16),
            pltpu.VMEM((NY, 2, 2, ST_ROWS, HEAD), BF16),
            pltpu.VMEM((2, 2 * TOK, HEAD), BF16),
            pltpu.VMEM((2, 2 * TOK, HEAD), F32),
            pltpu.VMEM((2, 2 * TOK, HEAD), F32),
            pltpu.VMEM((2, 2 * TOK, HEAD), F32),
            pltpu.VMEM((2, TOK, HEAD), F32),
            pltpu.VMEM((2, TOK, HEAD), BF16),
            pltpu.VMEM((2, NX, QUART, 2 * HEAD), BF16),
            pltpu.VMEM((NX, 2, QUART, 2 * HEAD), BF16),
            DMA((26,)),
            DMA((2,)), DMA((2,)), DMA((6,)), DMA((6,)), DMA((1,)), DMA((1,)),
            DMA((NZ - 1,)), DMA((NZ - 1,)), DMA((12,)), DMA((12,)), DMA((12,)), DMA((12,)),
            DMA((2 * NX,)), DMA((2 * NX,)), DMA((16,)), DMA((16,)),
            *ring_sems(4), *ring_sems(4), *ring_sems(2),
        ],
        compiler_params=pltpu.CompilerParams(
            collective_id=0, has_side_effects=True, vmem_limit_bytes=VMEM_LIMIT
        ),
    )(
        tokens_in.reshape(NX, QUART, d_model), rec_query_weight, rec_forget_weight, rec_input_weight,
        att_value_weight, att_query_weight, att_key_weight, recurrence_output_weight, out_att_weight,
        decay_shift, norm_gain[None], jnp.asarray(frequency), floor_gap.reshape(2, HEAD),
        rec_gain[None], att_gain[None], lambda_head,
    )
    return out.reshape(TOK, d_model)


def solution(mesh):
    split = Mesh(mesh.devices.reshape(NZ, NY, 2, NX), ("sp_0", "sp_1", "sp_2", "tp"))
    placed = (
        P(SP, None), P(), P(SP, "tp"), P(SP, "tp"), P(SP, "tp"), P(SP, "tp"), P(SP, "tp"), P(SP, "tp"),
        P("tp", None), P("tp", None), P("tp"), P("tp", SP), P(), P(), P("tp"),
    )
    return jax.shard_map(
        per_device, mesh=split, in_specs=placed, out_specs=P(SP, None), check_vma=False
    )
```

```python
import functools

import jax
import jax.numpy as jnp
import numpy as np
from jax import lax
from jax.experimental import pallas as pl
from jax.experimental.pallas import tpu as pltpu
from jax.sharding import Mesh
from jax.sharding import PartitionSpec as P

HEAD = 128
PAIR = 64
BLOCK = 64
SP = ("sp_0", "sp_1", "sp_2")
NZ, NY, NX = 8, 8, 4
HALF = NY // 2
TOK = 256
QUART = TOK // NX
ST_ROWS = 160
RECUR_EPSILON = 1e-06
ATTEND_EPSILON = 1e-05
ROTARY_BASE = 10000.0
SCORE_LOG2 = PAIR ** (-0.5) * 1.4426950408889634
F32, BF16 = jnp.float32, jnp.bfloat16
DMA = pltpu.SemaphoreType.DMA
VM = pl.BlockSpec(memory_space=pltpu.VMEM)
HBM = pl.BlockSpec(memory_space=pltpu.HBM)
OUT_HALF = 1024
VMEM_LIMIT = 60 * 1024 * 1024
REL = (0, 1, 7, 2, 6, 3, 5, 4)
POS = tuple(REL.index(d) for d in range(NZ))
MESH_ID = pl.DeviceIdType.MESH
NT = (((1,), (1,)), ((), ()))


def remote(src, dst, send, recv, where):
    return pltpu.make_async_remote_copy(
        src_ref=src, dst_ref=dst, send_sem=send, recv_sem=recv, device_id=where, device_id_type=MESH_ID
    )


def greet(places):
    barrier = pltpu.get_barrier_semaphore()
    for place in places:
        pl.semaphore_signal(barrier, inc=1, device_id=place, device_id_type=MESH_ID)
    pl.semaphore_wait(barrier, len(places))


def where_am_i():
    return (lax.axis_index("sp_0"), lax.axis_index("sp_1"), lax.axis_index("sp_2"), lax.axis_index("tp"))


def partner_row(z):
    return jnp.where(z % 2 == 1, (z + 1) % NZ, (z + NZ - 1) % NZ)


class Ring:
    def __init__(self, y, c, parts, piece, sems):
        self.y, self.c, self.parts, self.piece = y, c, parts, piece
        self.sr, self.rr, self.sl, self.rl, self.sp, self.rp = sems
        self.right = {"sp_1": (y + 1) % NY}
        self.left = {"sp_1": (y + NY - 1) % NY}
        self.other = {"sp_2": 1 - c}

    def at(self, offset, i):
        return self.piece((self.y + offset + NY) % NY, self.c, i)

    def index(self, k, i):
        return self.parts * (k - 1) + i

    def to_right(self, k, i):
        ref, n = self.at(1 - k, i), self.index(k, i)
        return remote(ref, ref, self.sr.at[n], self.rr.at[n], self.right)

    def to_left(self, k, i):
        ref, n = self.at(k - 1, i), self.index(k, i)
        return remote(ref, ref, self.sl.at[n], self.rl.at[n], self.left)

    def to_other(self, offset, i):
        ref, n = self.at(offset, i), self.parts * (offset % NY) + i
        return remote(ref, ref, self.sp.at[n], self.rp.at[n], self.other)

    def goes_right(self, k, i):
        return k < HALF or (k == HALF and i < self.parts // 2)

    def goes_left(self, k, i):
        return k < HALF or (k == HALF and i >= self.parts // 2)

    def begin(self, i):
        self.to_right(1, i).start()
        self.to_left(1, i).start()
        self.to_other(0, i).start()

    def step(self, k, i):
        n = self.index(k, i)
        if self.goes_right(k, i):
            ref = self.at(-k, i)
            remote(ref, ref, self.sr.at[n], self.rr.at[n], self.right).wait_recv()
            if self.goes_right(k + 1, i):
                self.to_right(k + 1, i).start()
            self.to_other(-k, i).start()
        if self.goes_left(k, i):
            ref = self.at(k, i)
            remote(ref, ref, self.sl.at[n], self.rl.at[n], self.left).wait_recv()
            if self.goes_left(k + 1, i):
                self.to_left(k + 1, i).start()
            self.to_other(k, i).start()

    def wait_other(self, offset):
        for i in range(self.parts):
            ref = self.piece((self.y + offset + NY) % NY, 1 - self.c, i)
            n = self.parts * (offset % NY) + i
            remote(ref, ref, self.sp.at[n], self.rp.at[n], self.other).wait_recv()

    def finish(self):
        for i in range(self.parts):
            for k in range(1, HALF + 1):
                if self.goes_right(k, i):
                    self.to_right(k, i).wait_send()
                if self.goes_left(k, i):
                    self.to_left(k, i).wait_send()
            for offset in range(NY):
                self.to_other(offset, i).wait_send()


def ring_sems(parts):
    return [DMA((parts * HALF,))] * 4 + [DMA((parts * NY,))] * 2


def layer_kernel(
    x_ref, wq_ref, wf_ref, wi_ref, wv_ref, waq_ref, wak_ref, wr_ref, wa_ref,
    ds_hbm, gain_hbm, freq_hbm, fg_hbm, rgain_hbm, again_hbm, lam_ref,
    res_ref,
    out_ref, ds_ref, gain_ref, freq_ref, fg_ref, rgain_ref, again_ref,
    xloc, xp, xn, wloc, wbuf, dsp, dso, wobuf,
    rec, kvbuf, stbuf, pair, q2, m_s, l_s, acc, local, qdec, give, gm, sums,
    load, t1s, t1r, t2s, t2r, dss, dsr, w1s, w1r, wos, wor, wops, wopr, ms, mr, put, prs, prr,
    *sems,
):
    z, y, c, x = where_am_i()
    zp = partner_row(z)
    row = (z + 1) % 2
    linked = jnp.logical_and(z != 0, z != NZ - 1)
    right, left, far = (x + 1) % NX, (x + NX - 1) % NX, (x + 2) % NX
    to_r, to_l, core = {"tp": right}, {"tp": left}, {"sp_2": 1 - c}
    half = QUART // 2
    halves = (pl.ds(0, half), pl.ds(half, half))
    pieces = tuple(pl.ds(i * (QUART // 4), QUART // 4) for i in range(4))

    loads = []

    def bring(src, dst):
        copy = pltpu.make_async_copy(src, dst, load.at[len(loads)])
        copy.start()
        loads.append(copy)
        return copy

    mine = pl.ds(pl.multiple_of(row * HEAD, HEAD), HEAD)
    yours = pl.ds(pl.multiple_of((1 - row) * HEAD, HEAD), HEAD)
    weight_refs = (wq_ref, wf_ref, wi_ref, wv_ref, waq_ref, wak_ref)
    own_w = [
        bring(ref.at[:, mine], wbuf.at[0, y, c, :, pl.ds(p * HEAD, HEAD)])
        for p, ref in enumerate(weight_refs)
    ]
    other_w = [
        bring(ref.at[:, yours], wloc.at[:, pl.ds(p * HEAD, HEAD)]) for p, ref in enumerate(weight_refs)
    ]
    quarter = bring(x_ref.at[x], xloc.at[x])
    rest_x = [bring(x_ref.at[(x + d) % NX], xloc.at[(x + d) % NX]) for d in range(1, NX)]
    own_wo = [
        bring(ref.at[:, pl.ds(h * OUT_HALF, OUT_HALF)], wobuf.at[x, h, pl.ds(r * 2 * HEAD, 2 * HEAD)])
        for h in range(2)
        for r, ref in enumerate((wr_ref, wa_ref))
    ]

    small = [
        bring(src, dst)
        for src, dst in (
            (ds_hbm, ds_ref), (gain_hbm, gain_ref), (freq_hbm, freq_ref), (fg_hbm, fg_ref),
            (rgain_hbm, rgain_ref), (again_hbm, again_ref),
        )
    ]
    greet(
        [{"sp_0": (z + d) % NZ} for d in range(1, NZ)]
        + [to_r, to_l]
        + [{"sp_1": (y + 1) % NY}, {"sp_1": (y + NY - 1) % NY}, core]
    )

    def to_row(d):
        src = wbuf.at[0, y, c] if d % 2 == 0 else wloc
        at = POS[(NZ - d) % NZ]
        return remote(
            src, wbuf.at[at, y, c], w1s.at[at - 1], w1r.at[at - 1], {"sp_0": (z + d) % NZ}
        )

    def row_came(at):
        ref = wbuf.at[at, y, c]
        remote(ref, ref, w1s.at[at - 1], w1r.at[at - 1], core).wait_recv()

    spread = {d: to_row(d) for d in range(1, NZ)}
    across = [
        remote(xloc.at[x, rows], xp.at[x, rows], t1s.at[i], t1r.at[i], {"sp_0": zp})
        for i, rows in enumerate(pieces)
    ]
    shifts = remote(ds_ref, dsp, dss.at[0], dsr.at[0], {"sp_0": zp})
    for copy in other_w:
        copy.wait()
    spread[1].start()
    spread[7].start()
    for copy in own_w:
        copy.wait()
    for d in (2, 6, 3, 5, 4):
        spread[d].start()
    quarter.wait()
    for copy in across:
        copy.start()
    for copy in small:
        copy.wait()
    shifts.start()

    for copy in own_wo:
        copy.wait()

    def wo_at(group, i):
        return wobuf.at[group, c, pl.ds(i * HEAD, HEAD)]

    wo_right = [remote(wo_at(x, i), wo_at(x, i), wos.at[i], wor.at[i], to_r) for i in range(4)]
    wo_left = [remote(wo_at(x, i), wo_at(x, i), wos.at[4 + i], wor.at[4 + i], to_l) for i in range(4)]
    wo_on_right = [
        remote(wo_at(left, i), wo_at(left, i), wos.at[8 + i], wor.at[8 + i], to_r) for i in (0, 1)
    ]
    wo_on_left = [
        remote(wo_at(right, i), wo_at(right, i), wos.at[8 + i], wor.at[8 + i], to_l) for i in (2, 3)
    ]
    wo_push = {
        (g, i): remote(
            wo_at((x + g) % NX, i),
            wo_at((x + g) % NX, i),
            wops.at[4 * (g - 1) + i],
            wopr.at[4 * (g - 1) + i],
            core,
        )
        for g in (1, 2, 3)
        for i in range(4)
    }

    def wo_came(group_offset, i, slot):
        ref = wo_at((x + group_offset) % NX, i)
        remote(ref, ref, wos.at[slot], wor.at[slot], to_r).wait_recv()
        wo_push[(group_offset, i)].start()

    wo_right[0].start()
    wo_left[2].start()

    w_ring = Ring(
        y, c, 4, lambda yo, stream, i: wbuf.at[pl.ds(2 * i, 2), yo, stream], sems[0:6]
    )

    def normed(source, kind, i):
        values = source[i].astype(F32)
        mean_sq = jnp.mean(values * values, axis=-1, keepdims=True)
        scale = lax.rsqrt(mean_sq + RECUR_EPSILON)
        for p in range(NZ):
            cols = pl.ds(pl.multiple_of(((z + REL[p]) % NZ) * 256, 256), 256)
            value = source[i, :, cols].astype(F32) * scale * gain_ref[:, cols]
            xn[kind, pl.ds(pl.multiple_of(i * QUART, QUART), QUART), pl.ds(p * 256, 256)] = value.astype(BF16)

    t2_right = [remote(xp.at[x, r], xp.at[x, r], t2s.at[i], t2r.at[i], to_r) for i, r in enumerate(pieces)]
    t2_left = [remote(xp.at[x, r], xp.at[x, r], t2s.at[4 + i], t2r.at[4 + i], to_l) for i, r in enumerate(pieces)]
    t2_on_right = [
        remote(xp.at[left, pieces[i]], xp.at[left, pieces[i]], t2s.at[8 + i], t2r.at[8 + i], to_r) for i in (0, 1)
    ]
    t2_on_left = [
        remote(xp.at[right, pieces[i]], xp.at[right, pieces[i]], t2s.at[8 + i], t2r.at[8 + i], to_l) for i in (2, 3)
    ]

    def t2_came(group, i, slot):
        ref = xp.at[group, pieces[i]]
        remote(ref, ref, t2s.at[slot], t2r.at[slot], to_r).wait_recv()

    for copy in rest_x:
        copy.wait()
    for i in range(NX):
        normed(xloc, row, i)
    row_came(1)
    w_ring.begin(0)
    for i in range(1, 4):
        row_came(2 * i)
        row_came(2 * i + 1)
        w_ring.begin(i)
    w_ring.step(1, 0)
    w_ring.step(1, 1)
    for i in range(4):
        across[i].wait_recv()
        t2_right[i].start()
        t2_left[i].start()
        if i < 2:
            w_ring.step(1, 2 + i)
        elif i == 2:
            w_ring.step(2, 0)
    w_ring.step(2, 1)
    for i in range(2):
        t2_came(left, i, i)
        t2_on_right[i].start()
        t2_came(right, 2 + i, 6 + i)
        t2_on_left[i].start()
        w_ring.step(2, 2 + i)
    for i in (1, 2, 3):
        wo_right[i].start()
    for i in (3, 0, 1):
        wo_left[i].start()
    for i in range(4):
        w_ring.step(3, i)
        if i == 0:
            normed(xp, 1 - row, x)
        elif i == 1:
            t2_came(left, 2, 2)
            t2_came(left, 3, 3)
            normed(xp, 1 - row, left)
        elif i == 2:
            t2_came(right, 0, 4)
            t2_came(right, 1, 5)
            normed(xp, 1 - row, right)
    for i in range(4):
        t2_came(far, i, 8 + i)
    normed(xp, 1 - row, far)
    wo_came(3, 0, 0)
    wo_on_right[0].start()
    wo_came(1, 2, 6)
    wo_on_left[0].start()

    lane = lax.broadcasted_iota(jnp.int32, (TOK, HEAD), 1)
    first = (lane % PAIR) < (PAIR // 2)
    place = (2 * y + c) * TOK + lax.broadcasted_iota(jnp.int32, (TOK, HEAD), 0)
    tables = []
    for kind in range(2):
        at = place if kind == 0 else place + jnp.where(linked, 2 * NY * TOK, 0)
        angle = at.astype(F32) * freq_ref[...]
        sine = jnp.sin(angle)
        tables.append((jnp.cos(angle), jnp.where(first, -sine, sine)))
        m_s[kind, pl.ds(0, TOK)] = tables[kind][0]
        l_s[kind, pl.ds(0, TOK)] = tables[kind][1]

    def turned(values, kind):
        swapped = jnp.where(
            first, pltpu.roll(values, HEAD - PAIR // 2, 1), pltpu.roll(values, PAIR // 2, 1)
        )
        return values * m_s[kind, pl.ds(0, TOK)] + swapped * l_s[kind, pl.ds(0, TOK)]

    shifts.wait_recv()
    dso[pl.ds(row, 1)] = ds_ref[pl.ds(row, 1)]
    dso[pl.ds(1 - row, 1)] = dsp[pl.ds(row, 1)]
    for i in range(4):
        w_ring.step(4, i)
    for offset in range(NY):
        w_ring.wait_other(offset)

    def projected(part, kind):
        weight = wbuf[:, :, :, :, pl.ds(part * 256, 256)].reshape(NZ * NY * 2 * 16, 256)
        out = jnp.dot(xn[kind], weight, preferred_element_type=F32)
        return out[:, :HEAD], out[:, HEAD:]

    half_rows = TOK // 2
    kv_ring = Ring(
        y,
        c,
        4,
        lambda yo, stream, i: kvbuf.at[yo, i // 2, stream, pl.ds((i % 2) * half_rows, half_rows)],
        sems[6:12],
    )
    st_ring = Ring(
        y, c, 2, lambda yo, stream, i: stbuf.at[yo, stream, pl.ds(i * ST_ROWS // 2, ST_ROWS // 2)], sems[12:18]
    )
    for kind in range(2):
        one, two = projected(2, kind)
        kvbuf[y, kind, c, :, pl.ds(0, HEAD)] = turned(two, kind).astype(BF16)
        query = turned(one, kind)
        q2[kind, pl.ds(0, TOK)] = jnp.where(lane < PAIR, query, 0.0).astype(BF16)
        q2[kind, pl.ds(TOK, TOK)] = jnp.where(lane >= PAIR, query, 0.0).astype(BF16)
        if kind == 1:
            kv_ring.begin(0)
            kv_ring.begin(1)
        one, two = projected(1, kind)
        kvbuf[y, kind, c, :, pl.ds(HEAD, HEAD)] = two.astype(BF16)
        rec[2, kind] = one.astype(BF16)
    for kind in range(2):
        one, two = projected(0, kind)
        rec[0, kind] = one.astype(BF16)
        rec[1, kind] = two.astype(BF16)
        if kind == 0:
            kv_ring.begin(2)
            kv_ring.begin(3)

    causal = lax.broadcasted_iota(jnp.int32, (BLOCK, BLOCK), 0) >= lax.broadcasted_iota(
        jnp.int32, (BLOCK, BLOCK), 1
    )
    tril = jnp.where(causal, 1.0, 0.0).astype(F32)
    gap = fg_ref[pl.ds(row, 1)]

    def segment(kind):
        shift = jnp.broadcast_to(dso[pl.ds(kind, 1)], (HEAD, TOK)).T
        state = jnp.zeros((HEAD, HEAD), F32)
        total = jnp.zeros((1, HEAD), F32)
        for b in range(TOK // BLOCK):
            rows = pl.ds(b * BLOCK, BLOCK)
            forget = rec[1, kind, rows].astype(F32)
            query = rec[0, kind, rows].astype(F32)
            value = rec[2, kind, rows]
            gate = gap * (1.0 / (1.0 + jnp.exp(forget)))
            decay = jnp.log1p(-gate) + shift[b * BLOCK : (b + 1) * BLOCK]
            cum = jnp.dot(tril, decay, precision=lax.Precision.HIGHEST, preferred_element_type=F32)
            end = cum[BLOCK - 1 :, :]
            q_dec = query * jnp.exp(cum)
            qdec[kind, rows] = (q_dec * jnp.exp(total)).astype(BF16)
            q_dec = q_dec.astype(BF16)
            k_grow = (gate * jnp.exp(-cum)).astype(BF16)
            scores = lax.dot_general(q_dec, k_grow, NT, preferred_element_type=F32)
            scores = jnp.where(causal, scores, 0.0).astype(BF16)
            out = jnp.dot(scores, value, preferred_element_type=F32)
            if b > 0:
                out = out + lax.dot_general(q_dec, state.astype(BF16), NT, preferred_element_type=F32)
            local[kind, rows] = out
            k_end = (gate * jnp.exp(end - cum)).astype(BF16)
            fresh = jnp.dot(value.astype(F32).T.astype(BF16), k_end, preferred_element_type=F32)
            state = state * jnp.exp(end) + fresh
            total = total + end
        pack(pair, (c, kind), state, total)

    def pack(buffer, where, state, total):
        buffer[(*where, pl.ds(0, HEAD))] = state.astype(BF16)
        high = total.astype(BF16)
        rest = total - high.astype(F32)
        middle = rest.astype(BF16)
        low = (rest - middle.astype(F32)).astype(BF16)
        index = lax.broadcasted_iota(jnp.int32, (ST_ROWS - HEAD, HEAD), 0)
        stack = jnp.where(
            index == 0, high.astype(F32), jnp.where(index == 1, middle.astype(F32), low.astype(F32))
        )
        buffer[(*where, pl.ds(HEAD, ST_ROWS - HEAD))] = stack.astype(BF16)

    def unpack(buffer, where):
        tail = buffer[(*where, pl.ds(HEAD, ST_ROWS - HEAD))].astype(F32)
        return buffer[(*where, pl.ds(0, HEAD))].astype(F32), tail[0:1] + tail[1:2] + tail[2:3]

    def pair_came(kind):
        ref = pair.at[1 - c, kind]
        remote(ref, ref, prs.at[kind], prr.at[kind], core).wait_recv()

    pair_sends = [
        remote(pair.at[c, kind], pair.at[c, kind], prs.at[kind], prr.at[kind], core) for kind in range(2)
    ]

    segment(0)
    pair_sends[0].start()
    segment(1)
    pair_sends[1].start()
    kv_ring.step(1, 0)
    kv_ring.step(1, 1)
    pair_came(0)
    pair_came(1)
    early, early_total = unpack(pair, (0, c))
    late, late_total = unpack(pair, (1, c))
    pack(stbuf, (y, c), early * jnp.exp(late_total) + late, early_total + late_total)
    st_ring.begin(0)
    st_ring.begin(1)

    def keys_values(yo, kind):
        both = kvbuf[yo, kind].reshape(2 * TOK, 2 * HEAD)
        return both[:, :HEAD], both[:, HEAD:]

    kv_ring.wait_other(0)

    ones = jnp.ones((2 * TOK, HEAD), BF16)

    def own(kind, carry):
        keys, values = keys_values(y, kind)
        values = jnp.concatenate([values, ones], axis=1)
        halves_of = [pl.ds(part * TOK, TOK) for part in range(2)]
        queries = [q2[kind, rows] for rows in halves_of]
        seen = lax.broadcasted_iota(jnp.int32, (TOK, 2 * TOK), 1) <= (
            lax.broadcasted_iota(jnp.int32, (TOK, 2 * TOK), 0) + c * TOK
        )
        done = []
        for query in queries:
            scores = lax.dot_general(query, keys, NT, preferred_element_type=F32)
            scores = jnp.where(seen, scores, -jnp.inf)
            best = jnp.broadcast_to(jnp.max(scores, axis=-1, keepdims=True), (TOK, HEAD))
            expo = jnp.exp2((scores - jnp.concatenate([best] * 4, axis=1)) * SCORE_LOG2).astype(BF16)
            done.append((best, jnp.dot(expo, values, preferred_element_type=F32)))
        for rows, (best, total) in zip(halves_of, done):
            m_s[kind, rows] = best
            acc[kind, rows] = total
        return carry

    lax.fori_loop(0, 2, own, 0)
    kv_ring.step(1, 2)
    kv_ring.step(1, 3)

    def absorb(yo, q_kind, kv_kind):
        keys, values = keys_values(yo, kv_kind)
        values = jnp.concatenate([values, ones], axis=1)
        halves_of = [pl.ds(part * TOK, TOK) for part in range(2)]
        queries = [q2[q_kind, rows] for rows in halves_of]
        olds = [m_s[q_kind, rows] for rows in halves_of]
        sums = [acc[q_kind, rows] for rows in halves_of]
        done = []
        for query, old, total in zip(queries, olds, sums):
            scores = lax.dot_general(query, keys, NT, preferred_element_type=F32)
            best = jnp.maximum(old, jnp.max(scores, axis=-1, keepdims=True))
            scale = jnp.exp2((old - best) * SCORE_LOG2)
            expo = jnp.exp2((scores - jnp.concatenate([best] * 4, axis=1)) * SCORE_LOG2).astype(BF16)
            fresh = jnp.dot(expo, values, preferred_element_type=F32)
            done.append((best, total * jnp.concatenate([scale] * 2, axis=1) + fresh))
        for rows, (best, total) in zip(halves_of, done):
            m_s[q_kind, rows] = best
            acc[q_kind, rows] = total

    def process(offset):
        if offset:
            kv_ring.wait_other(offset)
        yo = (y + offset + NY) % NY

        def unit(kind_at, carry):
            q_kind = jnp.where(kind_at == 0, 0, 1)
            kv_kind = jnp.where(kind_at == 2, 1, 0)
            wanted = jnp.where(kind_at == 1, linked.astype(jnp.int32), (yo < y).astype(jnp.int32))

            @pl.when(wanted == 1)
            def _():
                absorb(yo, q_kind, kv_kind)

            return carry

        lax.fori_loop(0, 3, unit, 0)

    process(0)
    for k in range(2, HALF + 1):
        kv_ring.step(k, 0)
        kv_ring.step(k, 1)
        process(1 - k)
        kv_ring.step(k, 2)
        kv_ring.step(k, 3)
        process(k - 1)
        st_ring.step(k - 1, 0)
        st_ring.step(k - 1, 1)
        if k == 2:
            wo_came(3, 1, 1)
            wo_on_right[1].start()
            wo_came(1, 3, 7)
            wo_on_left[1].start()
        elif k == 3:
            wo_came(3, 2, 2)
            wo_came(1, 0, 4)
        else:
            wo_came(3, 3, 3)
            wo_came(1, 1, 5)
            wo_came(2, 0, 8)
            wo_came(2, 2, 10)
    process(HALF)
    st_ring.step(HALF, 0)
    st_ring.step(HALF, 1)
    for offset in range(NY):
        st_ring.wait_other(offset)

    def pass_on(kind, yo, state):
        fresh, total = unpack(stbuf, (yo, kind))
        return state * jnp.exp(total) + fresh

    def within(kind, state):
        fresh, total = unpack(pair, (0, kind))
        after = state * jnp.exp(total) + fresh
        return jnp.where(c == 0, state, after)

    nothing = jnp.zeros((HEAD, HEAD), F32)
    into_low = lax.fori_loop(0, y, functools.partial(pass_on, 0), nothing)
    all_low = lax.fori_loop(y, NY, functools.partial(pass_on, 0), into_low)
    all_low = all_low * jnp.where(linked, 1.0, 0.0)
    into_high = lax.fori_loop(0, y, functools.partial(pass_on, 1), all_low)
    into_low, into_high = within(0, into_low), within(1, into_high)
    lam = lam_ref[row]
    token_halves = (pl.ds(0, TOK // 2), pl.ds(TOK // 2, TOK // 2))

    def mixed(kind):
        state = jnp.where(kind == 0, into_low, into_high).astype(BF16)
        raw = local[kind] + lax.dot_general(qdec[kind], state, NT, preferred_element_type=F32)
        mean_sq = jnp.mean(raw * raw, axis=-1, keepdims=True)
        rec_mix = (raw * lax.rsqrt(mean_sq + RECUR_EPSILON) * rgain_ref[...]).astype(BF16)
        low, high = acc[kind, pl.ds(0, TOK)], acc[kind, pl.ds(TOK, TOK)]
        raw = low[:, :HEAD] / low[:, HEAD:] - lam * (high[:, :HEAD] / high[:, HEAD:])
        mean_sq = jnp.mean(raw * raw, axis=-1, keepdims=True)
        att_mix = (raw * lax.rsqrt(mean_sq + ATTEND_EPSILON) * again_ref[...]).astype(BF16)
        return jnp.concatenate([rec_mix, att_mix], axis=1)

    def hop(group, head, i, slot, where):
        ref = gm.at[group, head, token_halves[i]]
        return remote(ref, ref, ms.at[slot], mr.at[slot], where)

    def came(group, head, i, slot):
        hop(group, head, i, slot, to_r).wait_recv()

    hops = []

    def go(*args):
        hops.append(hop(*args))
        hops[-1].start()

    give[...] = mixed(1 - row)
    gives = [
        remote(give.at[r], gm.at[x, row, r], ms.at[12 + i], mr.at[12 + i], {"sp_0": zp})
        for i, r in enumerate(token_halves)
    ]
    for copy in gives:
        copy.start()
    gm[x, row] = mixed(row)
    go(x, row, 0, 0, to_r)
    go(x, row, 1, 3, to_l)
    go(x, row, 1, 1, to_r)
    go(x, row, 0, 2, to_l)
    for i in range(2):
        came(x, 1 - row, i, 12 + i)
        go(x, 1 - row, i, 6 + i, to_r)
        go(x, 1 - row, i, 8 + i, to_l)

    def product(group, j):
        parts = [gm[group, h, :, pl.ds(p * HEAD, HEAD)] for p in range(2) for h in range(2)]
        weight = wobuf[group, j // 2, :, pl.ds((j % 2) * width, width)]
        out = jnp.dot(jnp.concatenate(parts, axis=1), weight, preferred_element_type=F32)
        return out.astype(BF16).astype(F32)

    def wo_ready(offset):
        for i in range(4):
            ref = wobuf.at[(x + offset) % NX, 1 - c, pl.ds(i * HEAD, HEAD)]
            n = 4 * (offset - 1) + i
            remote(ref, ref, wops.at[n], wopr.at[n], core).wait_recv()

    width = OUT_HALF // 2
    came(left, row, 0, 0)
    go(left, row, 0, 4, to_r)
    came(right, row, 1, 3)
    go(right, row, 1, 5, to_l)
    for j in range(4):
        sums[:, pl.ds(j * width, width)] = product(x, j)
    came(left, 1 - row, 0, 6)
    go(left, 1 - row, 0, 10, to_r)
    came(right, 1 - row, 1, 9)
    go(right, 1 - row, 1, 11, to_l)
    wo_came(2, 1, 9)
    wo_came(2, 3, 11)
    for offset in (1, 2, 3):
        wo_ready(offset)
    came(left, row, 1, 1)
    came(right, row, 0, 2)
    came(left, 1 - row, 1, 7)
    came(right, 1 - row, 0, 8)

    def near(i, carry):
        group = jnp.where(i == 0, left, right)
        for j in range(4):
            cols = pl.ds(j * width, width)
            sums[:, cols] = sums[:, cols] + product(group, j)
        return carry

    lax.fori_loop(0, 2, near, 0)
    came(far, row, 0, 4)
    came(far, row, 1, 5)
    came(far, 1 - row, 0, 10)
    came(far, 1 - row, 1, 11)
    puts = []
    for j in range(4):
        cols = pl.ds(j * width, width)
        out_ref[:, cols] = (sums[:, cols] + product(far, j)).astype(BF16)
        puts.append(pltpu.make_async_copy(out_ref.at[:, cols], res_ref.at[:, cols], put.at[j]))
        puts[-1].start()
    w_ring.finish()
    kv_ring.finish()
    st_ring.finish()
    sent = list(spread.values()) + across + [shifts] + t2_right + t2_left + t2_on_right + t2_on_left
    sent += wo_right + wo_left + wo_on_right + wo_on_left + list(wo_push.values()) + gives + hops + pair_sends
    for copy in sent:
        copy.wait_send()
    for copy in puts:
        copy.wait()


def per_device(
    tokens_in, norm_gain, rec_query_weight, rec_forget_weight, rec_input_weight, att_query_weight,
    att_key_weight, att_value_weight, recurrence_output_weight, out_att_weight, floor_gap,
    decay_shift, rec_gain, att_gain, lambda_head,
):
    width = PAIR // 2
    steps = np.arange(width, dtype=np.float32) / np.float32(width)
    frequency = np.float32(1.0) / np.float32(ROTARY_BASE) ** steps
    frequency = np.concatenate([frequency] * 4)[None].astype(np.float32)
    d_model = tokens_in.shape[1]
    return pl.pallas_call(
        layer_kernel,
        name="layer",
        out_shape=jax.ShapeDtypeStruct((TOK, d_model), BF16),
        in_specs=[HBM] * 15 + [pl.BlockSpec(memory_space=pltpu.SMEM)],
        out_specs=HBM,
        scratch_shapes=[
            pltpu.VMEM((TOK, d_model), BF16),
            pltpu.VMEM((2, TOK), F32),
            pltpu.VMEM((1, d_model), F32),
            pltpu.VMEM((1, HEAD), F32),
            pltpu.VMEM((2, HEAD), F32),
            pltpu.VMEM((1, HEAD), F32),
            pltpu.VMEM((1, HEAD), F32),
            pltpu.VMEM((NX, QUART, d_model), BF16),
            pltpu.VMEM((NX, QUART, d_model), BF16),
            pltpu.VMEM((2, TOK, d_model), BF16),
            pltpu.VMEM((16, 6 * HEAD), BF16),
            pltpu.VMEM((NZ, NY, 2, 16, 6 * HEAD), BF16),
            pltpu.VMEM((2, TOK), F32),
            pltpu.VMEM((2, TOK), F32),
            pltpu.VMEM((NX, 2, 4 * HEAD, OUT_HALF), BF16),
            pltpu.VMEM((3, 2, TOK, HEAD), BF16),
            pltpu.VMEM((NY, 2, 2, TOK, 2 * HEAD), BF16),
            pltpu.VMEM((NY, 2, ST_ROWS, HEAD), BF16),
            pltpu.VMEM((2, 2, ST_ROWS, HEAD), BF16),
            pltpu.VMEM((2, 2 * TOK, HEAD), BF16),
            pltpu.VMEM((2, 2 * TOK, HEAD), F32),
            pltpu.VMEM((2, TOK, HEAD), F32),
            pltpu.VMEM((2, 2 * TOK, 2 * HEAD), F32),
            pltpu.VMEM((2, TOK, HEAD), F32),
            pltpu.VMEM((2, TOK, HEAD), BF16),
            pltpu.VMEM((TOK, 2 * HEAD), BF16),
            pltpu.VMEM((NX, 2, TOK, 2 * HEAD), BF16),
            pltpu.VMEM((TOK, d_model), F32),
            DMA((26,)),
            DMA((4,)), DMA((4,)), DMA((12,)), DMA((12,)), DMA((1,)), DMA((1,)),
            DMA((NZ - 1,)), DMA((NZ - 1,)), DMA((12,)), DMA((12,)), DMA((12,)), DMA((12,)),
            DMA((14,)), DMA((14,)), DMA((4,)), DMA((2,)), DMA((2,)),
            *ring_sems(4), *ring_sems(4), *ring_sems(2),
        ],
        compiler_params=pltpu.CompilerParams(
            collective_id=0, has_side_effects=True, vmem_limit_bytes=VMEM_LIMIT
        ),
    )(
        tokens_in.reshape(NX, QUART, d_model), rec_query_weight, rec_forget_weight, rec_input_weight,
        att_value_weight, att_query_weight, att_key_weight, recurrence_output_weight, out_att_weight,
        decay_shift, norm_gain[None], jnp.asarray(frequency), floor_gap.reshape(2, HEAD),
        rec_gain[None], att_gain[None], lambda_head,
    )


def solution(mesh):
    split = Mesh(mesh.devices.reshape(NZ, NY, 2, NX), ("sp_0", "sp_1", "sp_2", "tp"))
    placed = (
        P(SP, None), P(), P(SP, "tp"), P(SP, "tp"), P(SP, "tp"), P(SP, "tp"), P(SP, "tp"), P(SP, "tp"),
        P("tp", None), P("tp", None), P("tp"), P("tp", SP), P(), P(), P("tp"),
    )
    return jax.shard_map(
        per_device, mesh=split, in_specs=placed, out_specs=P(SP, None), check_vma=False
    )
```

```python
import functools

import jax
import jax.numpy as jnp
import numpy as np
from jax import lax
from jax.experimental import pallas as pl
from jax.experimental.pallas import tpu as pltpu
from jax.sharding import Mesh
from jax.sharding import PartitionSpec as P

HEAD = 128
PAIR = 64
BLOCK = 64
SP = ("sp_0", "sp_1", "sp_2")
NZ, NY, NX = 8, 8, 4
HALF = NY // 2
TOK = 256
QUART = TOK // NX
ST_ROWS = 160
RECUR_EPSILON = 1e-06
ATTEND_EPSILON = 1e-05
ROTARY_BASE = 10000.0
SCORE_LOG2 = PAIR ** (-0.5) * 1.4426950408889634
F32, BF16 = jnp.float32, jnp.bfloat16
DMA = pltpu.SemaphoreType.DMA
VM = pl.BlockSpec(memory_space=pltpu.VMEM)
HBM = pl.BlockSpec(memory_space=pltpu.HBM)
OUT_HALF = 1024
VMEM_LIMIT = 60 * 1024 * 1024
REL = (0, 1, 7, 2, 6, 3, 5, 4)
POS = tuple(REL.index(d) for d in range(NZ))
MESH_ID = pl.DeviceIdType.MESH
NT = (((1,), (1,)), ((), ()))


def remote(src, dst, send, recv, where):
    return pltpu.make_async_remote_copy(
        src_ref=src, dst_ref=dst, send_sem=send, recv_sem=recv, device_id=where, device_id_type=MESH_ID
    )


def greet(places):
    barrier = pltpu.get_barrier_semaphore()
    for place in places:
        pl.semaphore_signal(barrier, inc=1, device_id=place, device_id_type=MESH_ID)
    pl.semaphore_wait(barrier, len(places))


def where_am_i():
    return (lax.axis_index("sp_0"), lax.axis_index("sp_1"), lax.axis_index("sp_2"), lax.axis_index("tp"))


def partner_row(z):
    return jnp.where(z % 2 == 1, (z + 1) % NZ, (z + NZ - 1) % NZ)


class Ring:
    def __init__(self, y, c, parts, piece, sems):
        self.y, self.c, self.parts, self.piece = y, c, parts, piece
        self.sr, self.rr, self.sl, self.rl, self.sp, self.rp = sems
        self.right = {"sp_1": (y + 1) % NY}
        self.left = {"sp_1": (y + NY - 1) % NY}
        self.other = {"sp_2": 1 - c}

    def at(self, offset, i):
        return self.piece((self.y + offset + NY) % NY, self.c, i)

    def index(self, k, i):
        return self.parts * (k - 1) + i

    def to_right(self, k, i):
        ref, n = self.at(1 - k, i), self.index(k, i)
        return remote(ref, ref, self.sr.at[n], self.rr.at[n], self.right)

    def to_left(self, k, i):
        ref, n = self.at(k - 1, i), self.index(k, i)
        return remote(ref, ref, self.sl.at[n], self.rl.at[n], self.left)

    def to_other(self, offset, i):
        ref, n = self.at(offset, i), self.parts * (offset % NY) + i
        return remote(ref, ref, self.sp.at[n], self.rp.at[n], self.other)

    def goes_right(self, k, i):
        return k < HALF or (k == HALF and i < self.parts // 2)

    def goes_left(self, k, i):
        return k < HALF or (k == HALF and i >= self.parts // 2)

    def begin(self, i):
        self.to_right(1, i).start()
        self.to_left(1, i).start()
        self.to_other(0, i).start()

    def step(self, k, i):
        n = self.index(k, i)
        if self.goes_right(k, i):
            ref = self.at(-k, i)
            remote(ref, ref, self.sr.at[n], self.rr.at[n], self.right).wait_recv()
            if self.goes_right(k + 1, i):
                self.to_right(k + 1, i).start()
            self.to_other(-k, i).start()
        if self.goes_left(k, i):
            ref = self.at(k, i)
            remote(ref, ref, self.sl.at[n], self.rl.at[n], self.left).wait_recv()
            if self.goes_left(k + 1, i):
                self.to_left(k + 1, i).start()
            self.to_other(k, i).start()

    def wait_other(self, offset):
        for i in range(self.parts):
            ref = self.piece((self.y + offset + NY) % NY, 1 - self.c, i)
            n = self.parts * (offset % NY) + i
            remote(ref, ref, self.sp.at[n], self.rp.at[n], self.other).wait_recv()

    def finish(self):
        for i in range(self.parts):
            for k in range(1, HALF + 1):
                if self.goes_right(k, i):
                    self.to_right(k, i).wait_send()
                if self.goes_left(k, i):
                    self.to_left(k, i).wait_send()
            for offset in range(NY):
                self.to_other(offset, i).wait_send()


def ring_sems(parts):
    return [DMA((parts * HALF,))] * 4 + [DMA((parts * NY,))] * 2


def layer_kernel(
    x_ref, wq_ref, wf_ref, wi_ref, wv_ref, waq_ref, wak_ref, wr_ref, wa_ref,
    ds_hbm, gain_hbm, freq_hbm, fg_hbm, rgain_hbm, again_hbm, lam_ref,
    res_ref,
    out_ref, ds_ref, gain_ref, freq_ref, fg_ref, rgain_ref, again_ref,
    xloc, xp, xn, wloc, wbuf, dsp, dso, wobuf,
    rec, kvbuf, stbuf, pair, q2, m_s, l_s, acc, local, qdec, give, gm, sums,
    load, t1s, t1r, t2s, t2r, dss, dsr, w1s, w1r, wos, wor, wops, wopr, ms, mr, put, prs, prr,
    *sems,
):
    z, y, c, x = where_am_i()
    zp = partner_row(z)
    row = (z + 1) % 2
    linked = jnp.logical_and(z != 0, z != NZ - 1)
    right, left, far = (x + 1) % NX, (x + NX - 1) % NX, (x + 2) % NX
    to_r, to_l, core = {"tp": right}, {"tp": left}, {"sp_2": 1 - c}
    half = QUART // 2
    halves = (pl.ds(0, half), pl.ds(half, half))
    pieces = tuple(pl.ds(i * (QUART // 4), QUART // 4) for i in range(4))

    loads = []

    def bring(src, dst):
        copy = pltpu.make_async_copy(src, dst, load.at[len(loads)])
        copy.start()
        loads.append(copy)
        return copy

    mine = pl.ds(pl.multiple_of(row * HEAD, HEAD), HEAD)
    yours = pl.ds(pl.multiple_of((1 - row) * HEAD, HEAD), HEAD)
    weight_refs = (wq_ref, wf_ref, wi_ref, wv_ref, waq_ref, wak_ref)
    own_w = [
        bring(ref.at[:, mine], wbuf.at[0, y, c, :, pl.ds(p * HEAD, HEAD)])
        for p, ref in enumerate(weight_refs)
    ]
    other_w = [
        bring(ref.at[:, yours], wloc.at[:, pl.ds(p * HEAD, HEAD)]) for p, ref in enumerate(weight_refs)
    ]
    quarter = bring(x_ref.at[x], xloc.at[x])
    rest_x = [bring(x_ref.at[(x + d) % NX], xloc.at[(x + d) % NX]) for d in range(1, NX)]
    own_wo = [
        bring(ref.at[:, pl.ds(h * OUT_HALF, OUT_HALF)], wobuf.at[x, h, pl.ds(r * 2 * HEAD, 2 * HEAD)])
        for h in range(2)
        for r, ref in enumerate((wr_ref, wa_ref))
    ]

    small = [
        bring(src, dst)
        for src, dst in (
            (ds_hbm, ds_ref), (gain_hbm, gain_ref), (freq_hbm, freq_ref), (fg_hbm, fg_ref),
            (rgain_hbm, rgain_ref), (again_hbm, again_ref),
        )
    ]
    greet(
        [{"sp_0": (z + d) % NZ} for d in range(1, NZ)]
        + [to_r, to_l]
        + [{"sp_1": (y + 1) % NY}, {"sp_1": (y + NY - 1) % NY}, core]
    )

    def to_row(d):
        src = wbuf.at[0, y, c] if d % 2 == 0 else wloc
        at = POS[(NZ - d) % NZ]
        return remote(
            src, wbuf.at[at, y, c], w1s.at[at - 1], w1r.at[at - 1], {"sp_0": (z + d) % NZ}
        )

    def row_came(at):
        ref = wbuf.at[at, y, c]
        remote(ref, ref, w1s.at[at - 1], w1r.at[at - 1], core).wait_recv()

    spread = {d: to_row(d) for d in range(1, NZ)}
    across = [
        remote(xloc.at[x, rows], xp.at[x, rows], t1s.at[i], t1r.at[i], {"sp_0": zp})
        for i, rows in enumerate(pieces)
    ]
    shifts = remote(ds_ref, dsp, dss.at[0], dsr.at[0], {"sp_0": zp})
    for copy in other_w:
        copy.wait()
    spread[1].start()
    spread[7].start()
    for copy in own_w:
        copy.wait()
    for d in (2, 6, 3, 5, 4):
        spread[d].start()
    quarter.wait()
    for copy in across:
        copy.start()
    for copy in small:
        copy.wait()
    shifts.start()

    for copy in own_wo:
        copy.wait()

    def wo_at(group, i):
        return wobuf.at[group, c, pl.ds(i * HEAD, HEAD)]

    wo_right = [remote(wo_at(x, i), wo_at(x, i), wos.at[i], wor.at[i], to_r) for i in range(4)]
    wo_left = [remote(wo_at(x, i), wo_at(x, i), wos.at[4 + i], wor.at[4 + i], to_l) for i in range(4)]
    wo_on_right = [
        remote(wo_at(left, i), wo_at(left, i), wos.at[8 + i], wor.at[8 + i], to_r) for i in (0, 1)
    ]
    wo_on_left = [
        remote(wo_at(right, i), wo_at(right, i), wos.at[8 + i], wor.at[8 + i], to_l) for i in (2, 3)
    ]
    wo_push = {
        (g, i): remote(
            wo_at((x + g) % NX, i),
            wo_at((x + g) % NX, i),
            wops.at[4 * (g - 1) + i],
            wopr.at[4 * (g - 1) + i],
            core,
        )
        for g in (1, 2, 3)
        for i in range(4)
    }

    def wo_came(group_offset, i, slot):
        ref = wo_at((x + group_offset) % NX, i)
        remote(ref, ref, wos.at[slot], wor.at[slot], to_r).wait_recv()
        wo_push[(group_offset, i)].start()

    wo_right[0].start()
    wo_left[2].start()

    w_ring = Ring(
        y, c, 4, lambda yo, stream, i: wbuf.at[pl.ds(2 * i, 2), yo, stream], sems[0:6]
    )

    def normed(source, kind, i):
        values = source[i].astype(F32)
        mean_sq = jnp.mean(values * values, axis=-1, keepdims=True)
        scale = lax.rsqrt(mean_sq + RECUR_EPSILON)
        for p in range(NZ):
            cols = pl.ds(pl.multiple_of(((z + REL[p]) % NZ) * 256, 256), 256)
            value = source[i, :, cols].astype(F32) * scale * gain_ref[:, cols]
            xn[kind, pl.ds(pl.multiple_of(i * QUART, QUART), QUART), pl.ds(p * 256, 256)] = value.astype(BF16)

    t2_right = [remote(xp.at[x, r], xp.at[x, r], t2s.at[i], t2r.at[i], to_r) for i, r in enumerate(pieces)]
    t2_left = [remote(xp.at[x, r], xp.at[x, r], t2s.at[4 + i], t2r.at[4 + i], to_l) for i, r in enumerate(pieces)]
    t2_on_right = [
        remote(xp.at[left, pieces[i]], xp.at[left, pieces[i]], t2s.at[8 + i], t2r.at[8 + i], to_r) for i in (0, 1)
    ]
    t2_on_left = [
        remote(xp.at[right, pieces[i]], xp.at[right, pieces[i]], t2s.at[8 + i], t2r.at[8 + i], to_l) for i in (2, 3)
    ]

    def t2_came(group, i, slot):
        ref = xp.at[group, pieces[i]]
        remote(ref, ref, t2s.at[slot], t2r.at[slot], to_r).wait_recv()

    for copy in rest_x:
        copy.wait()
    for i in range(NX):
        normed(xloc, row, i)
    row_came(1)
    w_ring.begin(0)
    for i in range(1, 3):
        row_came(2 * i)
        row_came(2 * i + 1)
        w_ring.begin(i)
    w_ring.step(1, 0)
    row_came(6)
    row_came(7)
    w_ring.begin(3)
    w_ring.step(1, 1)
    lane = lax.broadcasted_iota(jnp.int32, (TOK, HEAD), 1)
    first = (lane % PAIR) < (PAIR // 2)
    place = (2 * y + c) * TOK + lax.broadcasted_iota(jnp.int32, (TOK, HEAD), 0)
    tables = []
    for kind in range(2):
        at = place if kind == 0 else place + jnp.where(linked, 2 * NY * TOK, 0)
        angle = at.astype(F32) * freq_ref[...]
        sine = jnp.sin(angle)
        tables.append((jnp.cos(angle), jnp.where(first, -sine, sine)))
        m_s[kind, pl.ds(0, TOK)] = tables[kind][0]
        l_s[kind, pl.ds(0, TOK)] = tables[kind][1]

    def turned(values, kind):
        swapped = jnp.where(
            first, pltpu.roll(values, HEAD - PAIR // 2, 1), pltpu.roll(values, PAIR // 2, 1)
        )
        return values * m_s[kind, pl.ds(0, TOK)] + swapped * l_s[kind, pl.ds(0, TOK)]

    def tokens_came(i):
        across[i].wait_recv()
        t2_right[i].start()
        t2_left[i].start()

    def from_left(i):
        t2_came(left, i, i)
        t2_on_right[i].start()

    def from_right(i):
        t2_came(right, i, 4 + i)
        t2_on_left[i - 2].start()

    w_ring.step(1, 2)
    tokens_came(0)
    w_ring.step(1, 3)
    tokens_came(1)
    w_ring.step(2, 0)
    tokens_came(2)
    w_ring.step(2, 1)
    tokens_came(3)
    w_ring.step(2, 2)
    normed(xp, 1 - row, x)
    from_left(0)
    w_ring.step(2, 3)
    from_left(1)
    from_right(2)
    w_ring.step(3, 0)
    from_right(3)
    for i in (1, 2, 3):
        wo_right[i].start()
    for i in (3, 0, 1):
        wo_left[i].start()
    w_ring.step(3, 1)
    t2_came(left, 2, 2)
    t2_came(left, 3, 3)
    normed(xp, 1 - row, left)
    w_ring.step(3, 2)
    t2_came(right, 0, 4)
    t2_came(right, 1, 5)
    normed(xp, 1 - row, right)
    w_ring.step(3, 3)
    w_ring.step(4, 0)
    w_ring.step(4, 2)
    for i in range(4):
        t2_came(far, i, 8 + i)
    normed(xp, 1 - row, far)
    wo_came(3, 0, 0)
    wo_on_right[0].start()
    wo_came(1, 2, 6)
    wo_on_left[0].start()
    shifts.wait_recv()
    dso[pl.ds(row, 1)] = ds_ref[pl.ds(row, 1)]
    dso[pl.ds(1 - row, 1)] = dsp[pl.ds(row, 1)]
    w_ring.step(4, 1)
    w_ring.step(4, 3)
    for offset in range(NY):
        w_ring.wait_other(offset)

    def projected(part, kind):
        weight = wbuf[:, :, :, :, pl.ds(part * 256, 256)].reshape(NZ * NY * 2 * 16, 256)
        out = jnp.dot(xn[kind], weight, preferred_element_type=F32)
        return out[:, :HEAD], out[:, HEAD:]

    half_rows = TOK // 2
    kv_ring = Ring(
        y,
        c,
        4,
        lambda yo, stream, i: kvbuf.at[yo, i // 2, stream, pl.ds((i % 2) * half_rows, half_rows)],
        sems[6:12],
    )
    st_ring = Ring(
        y, c, 2, lambda yo, stream, i: stbuf.at[yo, stream, pl.ds(i * ST_ROWS // 2, ST_ROWS // 2)], sems[12:18]
    )
    for kind in range(2):
        one, two = projected(2, kind)
        kvbuf[y, kind, c, :, pl.ds(0, HEAD)] = turned(two, kind).astype(BF16)
        query = turned(one, kind)
        q2[kind, pl.ds(0, TOK)] = jnp.where(lane < PAIR, query, 0.0).astype(BF16)
        q2[kind, pl.ds(TOK, TOK)] = jnp.where(lane >= PAIR, query, 0.0).astype(BF16)
        one, two = projected(1, kind)
        kvbuf[y, kind, c, :, pl.ds(HEAD, HEAD)] = two.astype(BF16)
        rec[2, kind] = one.astype(BF16)
        if kind == 0:
            kv_ring.begin(0)
            kv_ring.begin(1)
    for kind in range(2):
        one, two = projected(0, kind)
        rec[0, kind] = one.astype(BF16)
        rec[1, kind] = two.astype(BF16)
        if kind == 0:
            kv_ring.begin(2)
            kv_ring.begin(3)

    causal = lax.broadcasted_iota(jnp.int32, (BLOCK, BLOCK), 0) >= lax.broadcasted_iota(
        jnp.int32, (BLOCK, BLOCK), 1
    )
    tril = jnp.where(causal, 1.0, 0.0).astype(F32)
    gap = fg_ref[pl.ds(row, 1)]

    def segment(kind):
        shift = jnp.broadcast_to(dso[pl.ds(kind, 1)], (HEAD, TOK)).T
        state = jnp.zeros((HEAD, HEAD), F32)
        total = jnp.zeros((1, HEAD), F32)
        for b in range(TOK // BLOCK):
            rows = pl.ds(b * BLOCK, BLOCK)
            forget = rec[1, kind, rows].astype(F32)
            query = rec[0, kind, rows].astype(F32)
            value = rec[2, kind, rows]
            gate = gap * (1.0 / (1.0 + jnp.exp(forget)))
            decay = jnp.log1p(-gate) + shift[b * BLOCK : (b + 1) * BLOCK]
            cum = jnp.dot(tril, decay, precision=lax.Precision.HIGHEST, preferred_element_type=F32)
            end = cum[BLOCK - 1 :, :]
            q_dec = query * jnp.exp(cum)
            qdec[kind, rows] = (q_dec * jnp.exp(total)).astype(BF16)
            q_dec = q_dec.astype(BF16)
            k_grow = (gate * jnp.exp(-cum)).astype(BF16)
            scores = lax.dot_general(q_dec, k_grow, NT, preferred_element_type=F32)
            scores = jnp.where(causal, scores, 0.0).astype(BF16)
            out = jnp.dot(scores, value, preferred_element_type=F32)
            if b > 0:
                out = out + lax.dot_general(q_dec, state.astype(BF16), NT, preferred_element_type=F32)
            local[kind, rows] = out
            k_end = (gate * jnp.exp(end - cum)).astype(BF16)
            fresh = jnp.dot(value.astype(F32).T.astype(BF16), k_end, preferred_element_type=F32)
            state = state * jnp.exp(end) + fresh
            total = total + end
        pack(pair, (c, kind), state, total)

    def pack(buffer, where, state, total):
        buffer[(*where, pl.ds(0, HEAD))] = state.astype(BF16)
        high = total.astype(BF16)
        rest = total - high.astype(F32)
        middle = rest.astype(BF16)
        low = (rest - middle.astype(F32)).astype(BF16)
        index = lax.broadcasted_iota(jnp.int32, (ST_ROWS - HEAD, HEAD), 0)
        stack = jnp.where(
            index == 0, high.astype(F32), jnp.where(index == 1, middle.astype(F32), low.astype(F32))
        )
        buffer[(*where, pl.ds(HEAD, ST_ROWS - HEAD))] = stack.astype(BF16)

    def unpack(buffer, where):
        tail = buffer[(*where, pl.ds(HEAD, ST_ROWS - HEAD))].astype(F32)
        return buffer[(*where, pl.ds(0, HEAD))].astype(F32), tail[0:1] + tail[1:2] + tail[2:3]

    def pair_came(kind):
        ref = pair.at[1 - c, kind]
        remote(ref, ref, prs.at[kind], prr.at[kind], core).wait_recv()

    pair_sends = [
        remote(pair.at[c, kind], pair.at[c, kind], prs.at[kind], prr.at[kind], core) for kind in range(2)
    ]

    segment(0)
    pair_sends[0].start()
    segment(1)
    pair_sends[1].start()
    kv_ring.step(1, 0)
    kv_ring.step(1, 1)
    def keys_values(yo, kind):
        both = kvbuf[yo, kind].reshape(2 * TOK, 2 * HEAD)
        return both[:, :HEAD], both[:, HEAD:]

    kv_ring.wait_other(0)

    ones = jnp.ones((2 * TOK, HEAD), BF16)

    def own(kind, carry):
        keys, values = keys_values(y, kind)
        values = jnp.concatenate([values, ones], axis=1)
        halves_of = [pl.ds(part * TOK, TOK) for part in range(2)]
        queries = [q2[kind, rows] for rows in halves_of]
        seen = lax.broadcasted_iota(jnp.int32, (TOK, 2 * TOK), 1) <= (
            lax.broadcasted_iota(jnp.int32, (TOK, 2 * TOK), 0) + c * TOK
        )
        done = []
        for query in queries:
            scores = lax.dot_general(query, keys, NT, preferred_element_type=F32)
            scores = jnp.where(seen, scores, -jnp.inf)
            best = jnp.broadcast_to(jnp.max(scores, axis=-1, keepdims=True), (TOK, HEAD))
            expo = jnp.exp2((scores - jnp.concatenate([best] * 4, axis=1)) * SCORE_LOG2).astype(BF16)
            done.append((best, jnp.dot(expo, values, preferred_element_type=F32)))
        for rows, (best, total) in zip(halves_of, done):
            m_s[kind, rows] = best
            acc[kind, rows] = total
        return carry

    lax.fori_loop(0, 2, own, 0)
    kv_ring.step(1, 2)
    kv_ring.step(1, 3)
    pair_came(0)
    pair_came(1)
    early, early_total = unpack(pair, (0, c))
    late, late_total = unpack(pair, (1, c))
    pack(stbuf, (y, c), early * jnp.exp(late_total) + late, early_total + late_total)
    st_ring.begin(0)
    st_ring.begin(1)

    def absorb(yo, q_kind, kv_kind):
        keys, values = keys_values(yo, kv_kind)
        values = jnp.concatenate([values, ones], axis=1)
        halves_of = [pl.ds(part * TOK, TOK) for part in range(2)]
        queries = [q2[q_kind, rows] for rows in halves_of]
        olds = [m_s[q_kind, rows] for rows in halves_of]
        sums = [acc[q_kind, rows] for rows in halves_of]
        done = []
        for query, old, total in zip(queries, olds, sums):
            scores = lax.dot_general(query, keys, NT, preferred_element_type=F32)
            best = jnp.maximum(old, jnp.max(scores, axis=-1, keepdims=True))
            scale = jnp.exp2((old - best) * SCORE_LOG2)
            expo = jnp.exp2((scores - jnp.concatenate([best] * 4, axis=1)) * SCORE_LOG2).astype(BF16)
            fresh = jnp.dot(expo, values, preferred_element_type=F32)
            done.append((best, total * jnp.concatenate([scale] * 2, axis=1) + fresh))
        for rows, (best, total) in zip(halves_of, done):
            m_s[q_kind, rows] = best
            acc[q_kind, rows] = total

    def process(offset):
        if offset:
            kv_ring.wait_other(offset)
        yo = (y + offset + NY) % NY

        def unit(kind_at, carry):
            q_kind = jnp.where(kind_at == 0, 0, 1)
            kv_kind = jnp.where(kind_at == 2, 1, 0)
            wanted = jnp.where(kind_at == 1, linked.astype(jnp.int32), (yo < y).astype(jnp.int32))

            @pl.when(wanted == 1)
            def _():
                absorb(yo, q_kind, kv_kind)

            return carry

        lax.fori_loop(0, 3, unit, 0)

    process(0)
    for k in range(2, HALF + 1):
        kv_ring.step(k, 0)
        kv_ring.step(k, 1)
        process(1 - k)
        kv_ring.step(k, 2)
        kv_ring.step(k, 3)
        process(k - 1)
        st_ring.step(k - 1, 0)
        st_ring.step(k - 1, 1)
        if k == 2:
            wo_came(3, 1, 1)
            wo_on_right[1].start()
            wo_came(1, 3, 7)
            wo_on_left[1].start()
        elif k == 3:
            wo_came(3, 2, 2)
            wo_came(1, 0, 4)
        else:
            wo_came(3, 3, 3)
            wo_came(1, 1, 5)
            wo_came(2, 0, 8)
            wo_came(2, 2, 10)
    process(HALF)
    st_ring.step(HALF, 0)
    st_ring.step(HALF, 1)
    for offset in range(NY):
        st_ring.wait_other(offset)

    def pass_on(kind, yo, state):
        fresh, total = unpack(stbuf, (yo, kind))
        return state * jnp.exp(total) + fresh

    def within(kind, state):
        fresh, total = unpack(pair, (0, kind))
        after = state * jnp.exp(total) + fresh
        return jnp.where(c == 0, state, after)

    nothing = jnp.zeros((HEAD, HEAD), F32)
    into_low = lax.fori_loop(0, y, functools.partial(pass_on, 0), nothing)
    all_low = lax.fori_loop(y, NY, functools.partial(pass_on, 0), into_low)
    all_low = all_low * jnp.where(linked, 1.0, 0.0)
    into_high = lax.fori_loop(0, y, functools.partial(pass_on, 1), all_low)
    into_low, into_high = within(0, into_low), within(1, into_high)
    lam = lam_ref[row]
    token_halves = (pl.ds(0, TOK // 2), pl.ds(TOK // 2, TOK // 2))

    def mixed(kind):
        state = jnp.where(kind == 0, into_low, into_high).astype(BF16)
        raw = local[kind] + lax.dot_general(qdec[kind], state, NT, preferred_element_type=F32)
        mean_sq = jnp.mean(raw * raw, axis=-1, keepdims=True)
        rec_mix = (raw * lax.rsqrt(mean_sq + RECUR_EPSILON) * rgain_ref[...]).astype(BF16)
        low, high = acc[kind, pl.ds(0, TOK)], acc[kind, pl.ds(TOK, TOK)]
        raw = low[:, :HEAD] / low[:, HEAD:] - lam * (high[:, :HEAD] / high[:, HEAD:])
        mean_sq = jnp.mean(raw * raw, axis=-1, keepdims=True)
        att_mix = (raw * lax.rsqrt(mean_sq + ATTEND_EPSILON) * again_ref[...]).astype(BF16)
        return jnp.concatenate([rec_mix, att_mix], axis=1)

    def hop(group, head, i, slot, where):
        ref = gm.at[group, head, token_halves[i]]
        return remote(ref, ref, ms.at[slot], mr.at[slot], where)

    def came(group, head, i, slot):
        hop(group, head, i, slot, to_r).wait_recv()

    hops = []

    def go(*args):
        hops.append(hop(*args))
        hops[-1].start()

    give[...] = mixed(1 - row)
    gives = [
        remote(give.at[r], gm.at[x, row, r], ms.at[12 + i], mr.at[12 + i], {"sp_0": zp})
        for i, r in enumerate(token_halves)
    ]
    for copy in gives:
        copy.start()
    gm[x, row] = mixed(row)
    go(x, row, 0, 0, to_r)
    go(x, row, 1, 3, to_l)
    go(x, row, 1, 1, to_r)
    go(x, row, 0, 2, to_l)
    for i in range(2):
        came(x, 1 - row, i, 12 + i)
        go(x, 1 - row, i, 6 + i, to_r)
        go(x, 1 - row, i, 8 + i, to_l)

    def product(group, j):
        parts = [gm[group, h, :, pl.ds(p * HEAD, HEAD)] for p in range(2) for h in range(2)]
        weight = wobuf[group, j // 2, :, pl.ds((j % 2) * width, width)]
        out = jnp.dot(jnp.concatenate(parts, axis=1), weight, preferred_element_type=F32)
        return out.astype(BF16).astype(F32)

    def wo_ready(offset):
        for i in range(4):
            ref = wobuf.at[(x + offset) % NX, 1 - c, pl.ds(i * HEAD, HEAD)]
            n = 4 * (offset - 1) + i
            remote(ref, ref, wops.at[n], wopr.at[n], core).wait_recv()

    width = OUT_HALF // 2
    came(left, row, 0, 0)
    go(left, row, 0, 4, to_r)
    came(right, row, 1, 3)
    go(right, row, 1, 5, to_l)
    for j in range(4):
        sums[:, pl.ds(j * width, width)] = product(x, j)
    came(left, 1 - row, 0, 6)
    go(left, 1 - row, 0, 10, to_r)
    came(right, 1 - row, 1, 9)
    go(right, 1 - row, 1, 11, to_l)
    wo_came(2, 1, 9)
    wo_came(2, 3, 11)
    for offset in (1, 2, 3):
        wo_ready(offset)
    came(left, row, 1, 1)
    came(right, row, 0, 2)
    came(left, 1 - row, 1, 7)
    came(right, 1 - row, 0, 8)

    def near(i, carry):
        group = jnp.where(i == 0, left, right)
        for j in range(4):
            cols = pl.ds(j * width, width)
            sums[:, cols] = sums[:, cols] + product(group, j)
        return carry

    lax.fori_loop(0, 2, near, 0)
    came(far, row, 0, 4)
    came(far, row, 1, 5)
    came(far, 1 - row, 0, 10)
    came(far, 1 - row, 1, 11)
    puts = []
    for j in range(4):
        cols = pl.ds(j * width, width)
        out_ref[:, cols] = (sums[:, cols] + product(far, j)).astype(BF16)
        puts.append(pltpu.make_async_copy(out_ref.at[:, cols], res_ref.at[:, cols], put.at[j]))
        puts[-1].start()
    w_ring.finish()
    kv_ring.finish()
    st_ring.finish()
    sent = list(spread.values()) + across + [shifts] + t2_right + t2_left + t2_on_right + t2_on_left
    sent += wo_right + wo_left + wo_on_right + wo_on_left + list(wo_push.values()) + gives + hops + pair_sends
    for copy in sent:
        copy.wait_send()
    for copy in puts:
        copy.wait()


def per_device(
    tokens_in, norm_gain, rec_query_weight, rec_forget_weight, rec_input_weight, att_query_weight,
    att_key_weight, att_value_weight, recurrence_output_weight, out_att_weight, floor_gap,
    decay_shift, rec_gain, att_gain, lambda_head,
):
    width = PAIR // 2
    steps = np.arange(width, dtype=np.float32) / np.float32(width)
    frequency = np.float32(1.0) / np.float32(ROTARY_BASE) ** steps
    frequency = np.concatenate([frequency] * 4)[None].astype(np.float32)
    d_model = tokens_in.shape[1]
    return pl.pallas_call(
        layer_kernel,
        name="layer",
        out_shape=jax.ShapeDtypeStruct((TOK, d_model), BF16),
        in_specs=[HBM] * 15 + [pl.BlockSpec(memory_space=pltpu.SMEM)],
        out_specs=HBM,
        scratch_shapes=[
            pltpu.VMEM((TOK, d_model), BF16),
            pltpu.VMEM((2, TOK), F32),
            pltpu.VMEM((1, d_model), F32),
            pltpu.VMEM((1, HEAD), F32),
            pltpu.VMEM((2, HEAD), F32),
            pltpu.VMEM((1, HEAD), F32),
            pltpu.VMEM((1, HEAD), F32),
            pltpu.VMEM((NX, QUART, d_model), BF16),
            pltpu.VMEM((NX, QUART, d_model), BF16),
            pltpu.VMEM((2, TOK, d_model), BF16),
            pltpu.VMEM((16, 6 * HEAD), BF16),
            pltpu.VMEM((NZ, NY, 2, 16, 6 * HEAD), BF16),
            pltpu.VMEM((2, TOK), F32),
            pltpu.VMEM((2, TOK), F32),
            pltpu.VMEM((NX, 2, 4 * HEAD, OUT_HALF), BF16),
            pltpu.VMEM((3, 2, TOK, HEAD), BF16),
            pltpu.VMEM((NY, 2, 2, TOK, 2 * HEAD), BF16),
            pltpu.VMEM((NY, 2, ST_ROWS, HEAD), BF16),
            pltpu.VMEM((2, 2, ST_ROWS, HEAD), BF16),
            pltpu.VMEM((2, 2 * TOK, HEAD), BF16),
            pltpu.VMEM((2, 2 * TOK, HEAD), F32),
            pltpu.VMEM((2, TOK, HEAD), F32),
            pltpu.VMEM((2, 2 * TOK, 2 * HEAD), F32),
            pltpu.VMEM((2, TOK, HEAD), F32),
            pltpu.VMEM((2, TOK, HEAD), BF16),
            pltpu.VMEM((TOK, 2 * HEAD), BF16),
            pltpu.VMEM((NX, 2, TOK, 2 * HEAD), BF16),
            pltpu.VMEM((TOK, d_model), F32),
            DMA((26,)),
            DMA((4,)), DMA((4,)), DMA((12,)), DMA((12,)), DMA((1,)), DMA((1,)),
            DMA((NZ - 1,)), DMA((NZ - 1,)), DMA((12,)), DMA((12,)), DMA((12,)), DMA((12,)),
            DMA((14,)), DMA((14,)), DMA((4,)), DMA((2,)), DMA((2,)),
            *ring_sems(4), *ring_sems(4), *ring_sems(2),
        ],
        compiler_params=pltpu.CompilerParams(
            collective_id=0, has_side_effects=True, vmem_limit_bytes=VMEM_LIMIT
        ),
    )(
        tokens_in.reshape(NX, QUART, d_model), rec_query_weight, rec_forget_weight, rec_input_weight,
        att_value_weight, att_query_weight, att_key_weight, recurrence_output_weight, out_att_weight,
        decay_shift, norm_gain[None], jnp.asarray(frequency), floor_gap.reshape(2, HEAD),
        rec_gain[None], att_gain[None], lambda_head,
    )


def solution(mesh):
    split = Mesh(mesh.devices.reshape(NZ, NY, 2, NX), ("sp_0", "sp_1", "sp_2", "tp"))
    placed = (
        P(SP, None), P(), P(SP, "tp"), P(SP, "tp"), P(SP, "tp"), P(SP, "tp"), P(SP, "tp"), P(SP, "tp"),
        P("tp", None), P("tp", None), P("tp"), P("tp", SP), P(), P(), P("tp"),
    )
    return jax.shard_map(
        per_device, mesh=split, in_specs=placed, out_specs=P(SP, None), check_vma=False
    )
```

```python
import functools

import jax
import jax.numpy as jnp
import numpy as np
from jax import lax
from jax.experimental import pallas as pl
from jax.experimental.pallas import tpu as pltpu
from jax.sharding import Mesh
from jax.sharding import PartitionSpec as P

HEAD = 128
PAIR = 64
BLOCK = 64
SP = ("sp_0", "sp_1", "sp_2")
NZ, NY, NX = 8, 8, 4
HALF = NY // 2
TOK = 256
QUART = TOK // NX
ST_ROWS = 160
RECUR_EPSILON = 1e-06
ATTEND_EPSILON = 1e-05
ROTARY_BASE = 10000.0
SCORE_LOG2 = PAIR ** (-0.5) * 1.4426950408889634
F32, BF16 = jnp.float32, jnp.bfloat16
DMA = pltpu.SemaphoreType.DMA
VM = pl.BlockSpec(memory_space=pltpu.VMEM)
HBM = pl.BlockSpec(memory_space=pltpu.HBM)
OUT_HALF = 1024
VMEM_LIMIT = 60 * 1024 * 1024
REL = (0, 1, 7, 2, 6, 3, 5, 4)
POS = tuple(REL.index(d) for d in range(NZ))
MESH_ID = pl.DeviceIdType.MESH
NT = (((1,), (1,)), ((), ()))


def remote(src, dst, send, recv, where):
    return pltpu.make_async_remote_copy(
        src_ref=src, dst_ref=dst, send_sem=send, recv_sem=recv, device_id=where, device_id_type=MESH_ID
    )


def greet(places):
    barrier = pltpu.get_barrier_semaphore()
    for place in places:
        pl.semaphore_signal(barrier, inc=1, device_id=place, device_id_type=MESH_ID)
    pl.semaphore_wait(barrier, len(places))


def where_am_i():
    return (lax.axis_index("sp_0"), lax.axis_index("sp_1"), lax.axis_index("sp_2"), lax.axis_index("tp"))


def partner_row(z):
    return jnp.where(z % 2 == 1, (z + 1) % NZ, (z + NZ - 1) % NZ)


class Ring:
    def __init__(self, y, c, parts, piece, sems):
        self.y, self.c, self.parts, self.piece = y, c, parts, piece
        self.sr, self.rr, self.sl, self.rl, self.sp, self.rp = sems
        self.right = {"sp_1": (y + 1) % NY}
        self.left = {"sp_1": (y + NY - 1) % NY}
        self.other = {"sp_2": 1 - c}

    def at(self, offset, i):
        return self.piece((self.y + offset + NY) % NY, self.c, i)

    def index(self, k, i):
        return self.parts * (k - 1) + i

    def to_right(self, k, i):
        ref, n = self.at(1 - k, i), self.index(k, i)
        return remote(ref, ref, self.sr.at[n], self.rr.at[n], self.right)

    def to_left(self, k, i):
        ref, n = self.at(k - 1, i), self.index(k, i)
        return remote(ref, ref, self.sl.at[n], self.rl.at[n], self.left)

    def to_other(self, offset, i):
        ref, n = self.at(offset, i), self.parts * (offset % NY) + i
        return remote(ref, ref, self.sp.at[n], self.rp.at[n], self.other)

    def goes_right(self, k, i):
        return k < HALF or (k == HALF and i < self.parts // 2)

    def goes_left(self, k, i):
        return k < HALF or (k == HALF and i >= self.parts // 2)

    def begin(self, i):
        self.to_right(1, i).start()
        self.to_left(1, i).start()
        self.to_other(0, i).start()

    def step(self, k, i):
        n = self.index(k, i)
        if self.goes_right(k, i):
            ref = self.at(-k, i)
            remote(ref, ref, self.sr.at[n], self.rr.at[n], self.right).wait_recv()
            if self.goes_right(k + 1, i):
                self.to_right(k + 1, i).start()
            self.to_other(-k, i).start()
        if self.goes_left(k, i):
            ref = self.at(k, i)
            remote(ref, ref, self.sl.at[n], self.rl.at[n], self.left).wait_recv()
            if self.goes_left(k + 1, i):
                self.to_left(k + 1, i).start()
            self.to_other(k, i).start()

    def wait_other(self, offset):
        for i in range(self.parts):
            ref = self.piece((self.y + offset + NY) % NY, 1 - self.c, i)
            n = self.parts * (offset % NY) + i
            remote(ref, ref, self.sp.at[n], self.rp.at[n], self.other).wait_recv()

    def finish(self):
        for i in range(self.parts):
            for k in range(1, HALF + 1):
                if self.goes_right(k, i):
                    self.to_right(k, i).wait_send()
                if self.goes_left(k, i):
                    self.to_left(k, i).wait_send()
            for offset in range(NY):
                self.to_other(offset, i).wait_send()


def ring_sems(parts):
    return [DMA((parts * HALF,))] * 4 + [DMA((parts * NY,))] * 2


def layer_kernel(
    x_ref, wq_ref, wf_ref, wi_ref, wv_ref, waq_ref, wak_ref, wr_ref, wa_ref,
    ds_hbm, gain_hbm, freq_hbm, fg_hbm, rgain_hbm, again_hbm, lam_ref,
    res_ref,
    out_ref, ds_ref, gain_ref, freq_ref, fg_ref, rgain_ref, again_ref,
    xloc, xp, xn, wloc, wbuf, dsp, dso, wobuf,
    rec, kvbuf, stbuf, pair, q2, m_s, l_s, acc, local, qdec, give, gm, sums,
    load, t1s, t1r, t2s, t2r, dss, dsr, w1s, w1r, wos, wor, wops, wopr, ms, mr, put, prs, prr,
    *sems,
):
    z, y, c, x = where_am_i()
    zp = partner_row(z)
    row = (z + 1) % 2
    linked = jnp.logical_and(z != 0, z != NZ - 1)
    right, left, far = (x + 1) % NX, (x + NX - 1) % NX, (x + 2) % NX
    to_r, to_l, core = {"tp": right}, {"tp": left}, {"sp_2": 1 - c}
    half = QUART // 2
    halves = (pl.ds(0, half), pl.ds(half, half))
    pieces = tuple(pl.ds(i * (QUART // 4), QUART // 4) for i in range(4))

    loads = []

    def bring(src, dst):
        copy = pltpu.make_async_copy(src, dst, load.at[len(loads)])
        copy.start()
        loads.append(copy)
        return copy

    mine = pl.ds(pl.multiple_of(row * HEAD, HEAD), HEAD)
    yours = pl.ds(pl.multiple_of((1 - row) * HEAD, HEAD), HEAD)
    weight_refs = (wq_ref, wf_ref, wi_ref, wv_ref, waq_ref, wak_ref)
    own_w = [
        bring(ref.at[:, mine], wbuf.at[0, y, c, :, pl.ds(p * HEAD, HEAD)])
        for p, ref in enumerate(weight_refs)
    ]
    other_w = [
        bring(ref.at[:, yours], wloc.at[:, pl.ds(p * HEAD, HEAD)]) for p, ref in enumerate(weight_refs)
    ]
    quarter = bring(x_ref.at[x], xloc.at[x])
    rest_x = [bring(x_ref.at[(x + d) % NX], xloc.at[(x + d) % NX]) for d in range(1, NX)]
    own_wo = [
        bring(ref.at[:, pl.ds(h * OUT_HALF, OUT_HALF)], wobuf.at[x, h, pl.ds(r * 2 * HEAD, 2 * HEAD)])
        for h in range(2)
        for r, ref in enumerate((wr_ref, wa_ref))
    ]

    small = [
        bring(src, dst)
        for src, dst in (
            (ds_hbm, ds_ref), (gain_hbm, gain_ref), (freq_hbm, freq_ref), (fg_hbm, fg_ref),
            (rgain_hbm, rgain_ref), (again_hbm, again_ref),
        )
    ]
    greet(
        [{"sp_0": (z + d) % NZ} for d in range(1, NZ)]
        + [to_r, to_l]
        + [{"sp_1": (y + 1) % NY}, {"sp_1": (y + NY - 1) % NY}, core]
    )

    def to_row(d):
        src = wbuf.at[0, y, c] if d % 2 == 0 else wloc
        at = POS[(NZ - d) % NZ]
        return remote(
            src, wbuf.at[at, y, c], w1s.at[at - 1], w1r.at[at - 1], {"sp_0": (z + d) % NZ}
        )

    def row_came(at):
        ref = wbuf.at[at, y, c]
        remote(ref, ref, w1s.at[at - 1], w1r.at[at - 1], core).wait_recv()

    spread = {d: to_row(d) for d in range(1, NZ)}
    across = [
        remote(xloc.at[x, rows], xp.at[x, rows], t1s.at[i], t1r.at[i], {"sp_0": zp})
        for i, rows in enumerate(pieces)
    ]
    shifts = remote(ds_ref, dsp, dss.at[0], dsr.at[0], {"sp_0": zp})
    for copy in other_w:
        copy.wait()
    spread[1].start()
    spread[7].start()
    for copy in own_w:
        copy.wait()
    for d in (2, 6, 3, 5, 4):
        spread[d].start()
    quarter.wait()
    for copy in across:
        copy.start()
    for copy in small:
        copy.wait()
    shifts.start()

    for copy in own_wo:
        copy.wait()

    def wo_at(group, i):
        return wobuf.at[group, c, pl.ds(i * HEAD, HEAD)]

    wo_right = [remote(wo_at(x, i), wo_at(x, i), wos.at[i], wor.at[i], to_r) for i in range(4)]
    wo_left = [remote(wo_at(x, i), wo_at(x, i), wos.at[4 + i], wor.at[4 + i], to_l) for i in range(4)]
    wo_on_right = [
        remote(wo_at(left, i), wo_at(left, i), wos.at[8 + i], wor.at[8 + i], to_r) for i in (0, 1)
    ]
    wo_on_left = [
        remote(wo_at(right, i), wo_at(right, i), wos.at[8 + i], wor.at[8 + i], to_l) for i in (2, 3)
    ]
    wo_push = {
        (g, i): remote(
            wo_at((x + g) % NX, i),
            wo_at((x + g) % NX, i),
            wops.at[4 * (g - 1) + i],
            wopr.at[4 * (g - 1) + i],
            core,
        )
        for g in (1, 2, 3)
        for i in range(4)
    }

    def wo_came(group_offset, i, slot):
        ref = wo_at((x + group_offset) % NX, i)
        remote(ref, ref, wos.at[slot], wor.at[slot], to_r).wait_recv()
        wo_push[(group_offset, i)].start()

    wo_right[0].start()
    wo_left[2].start()

    w_ring = Ring(
        y, c, 4, lambda yo, stream, i: wbuf.at[pl.ds(2 * i, 2), yo, stream], sems[0:6]
    )

    def normed(source, kind, i):
        values = source[i].astype(F32)
        mean_sq = jnp.mean(values * values, axis=-1, keepdims=True)
        scale = lax.rsqrt(mean_sq + RECUR_EPSILON)
        for p in range(NZ):
            cols = pl.ds(pl.multiple_of(((z + REL[p]) % NZ) * 256, 256), 256)
            value = source[i, :, cols].astype(F32) * scale * gain_ref[:, cols]
            xn[kind, pl.ds(pl.multiple_of(i * QUART, QUART), QUART), pl.ds(p * 256, 256)] = value.astype(BF16)

    t2_right = [remote(xp.at[x, r], xp.at[x, r], t2s.at[i], t2r.at[i], to_r) for i, r in enumerate(pieces)]
    t2_left = [remote(xp.at[x, r], xp.at[x, r], t2s.at[4 + i], t2r.at[4 + i], to_l) for i, r in enumerate(pieces)]
    t2_on_right = [
        remote(xp.at[left, pieces[i]], xp.at[left, pieces[i]], t2s.at[8 + i], t2r.at[8 + i], to_r) for i in (0, 1)
    ]
    t2_on_left = [
        remote(xp.at[right, pieces[i]], xp.at[right, pieces[i]], t2s.at[8 + i], t2r.at[8 + i], to_l) for i in (2, 3)
    ]

    def t2_came(group, i, slot):
        ref = xp.at[group, pieces[i]]
        remote(ref, ref, t2s.at[slot], t2r.at[slot], to_r).wait_recv()

    for copy in rest_x:
        copy.wait()
    for i in range(NX):
        normed(xloc, row, i)
    row_came(1)
    w_ring.begin(0)
    for i in range(1, 3):
        row_came(2 * i)
        row_came(2 * i + 1)
        w_ring.begin(i)
    w_ring.step(1, 0)
    row_came(6)
    row_came(7)
    w_ring.begin(3)
    w_ring.step(1, 1)
    lane = lax.broadcasted_iota(jnp.int32, (TOK, HEAD), 1)
    first = (lane % PAIR) < (PAIR // 2)
    place = (2 * y + c) * TOK + lax.broadcasted_iota(jnp.int32, (TOK, HEAD), 0)
    tables = []
    for kind in range(2):
        at = place if kind == 0 else place + jnp.where(linked, 2 * NY * TOK, 0)
        angle = at.astype(F32) * freq_ref[...]
        sine = jnp.sin(angle)
        tables.append((jnp.cos(angle), jnp.where(first, -sine, sine)))
        m_s[kind, pl.ds(0, TOK)] = tables[kind][0]
        l_s[kind, pl.ds(0, TOK)] = tables[kind][1]

    def turned(values, kind):
        swapped = jnp.where(
            first, pltpu.roll(values, HEAD - PAIR // 2, 1), pltpu.roll(values, PAIR // 2, 1)
        )
        return values * m_s[kind, pl.ds(0, TOK)] + swapped * l_s[kind, pl.ds(0, TOK)]

    def tokens_came(i):
        across[i].wait_recv()
        t2_right[i].start()
        t2_left[i].start()

    def from_left(i):
        t2_came(left, i, i)
        t2_on_right[i].start()

    def from_right(i):
        t2_came(right, i, 4 + i)
        t2_on_left[i - 2].start()

    w_ring.step(1, 2)
    tokens_came(0)
    w_ring.step(1, 3)
    tokens_came(1)
    w_ring.step(2, 0)
    tokens_came(2)
    w_ring.step(2, 1)
    tokens_came(3)
    w_ring.step(2, 2)
    normed(xp, 1 - row, x)
    from_left(0)
    w_ring.step(2, 3)
    from_left(1)
    from_right(2)
    w_ring.step(3, 0)
    from_right(3)
    for i in (1, 2, 3):
        wo_right[i].start()
    for i in (3, 0, 1):
        wo_left[i].start()
    w_ring.step(3, 1)
    t2_came(left, 2, 2)
    t2_came(left, 3, 3)
    normed(xp, 1 - row, left)
    w_ring.step(3, 2)
    t2_came(right, 0, 4)
    t2_came(right, 1, 5)
    normed(xp, 1 - row, right)
    w_ring.step(3, 3)
    w_ring.step(4, 0)
    w_ring.step(4, 2)
    for i in range(4):
        t2_came(far, i, 8 + i)
    normed(xp, 1 - row, far)
    wo_came(3, 0, 0)
    wo_on_right[0].start()
    wo_came(1, 2, 6)
    wo_on_left[0].start()
    shifts.wait_recv()
    dso[pl.ds(row, 1)] = ds_ref[pl.ds(row, 1)]
    dso[pl.ds(1 - row, 1)] = dsp[pl.ds(row, 1)]
    w_ring.step(4, 1)
    w_ring.step(4, 3)
    for offset in range(NY):
        w_ring.wait_other(offset)

    def projected(part, kind):
        weight = wbuf[:, :, :, :, pl.ds(part * 256, 256)].reshape(NZ * NY * 2 * 16, 256)
        out = jnp.dot(xn[kind], weight, preferred_element_type=F32)
        return out[:, :HEAD], out[:, HEAD:]

    half_rows = TOK // 2
    kv_ring = Ring(
        y,
        c,
        4,
        lambda yo, stream, i: kvbuf.at[yo, i // 2, stream, pl.ds((i % 2) * half_rows, half_rows)],
        sems[6:12],
    )
    st_ring = Ring(
        y, c, 2, lambda yo, stream, i: stbuf.at[yo, stream, pl.ds(i * ST_ROWS // 2, ST_ROWS // 2)], sems[12:18]
    )
    for kind in range(2):
        one, two = projected(2, kind)
        kvbuf[y, kind, c, :, pl.ds(0, HEAD)] = turned(two, kind).astype(BF16)
        query = turned(one, kind)
        q2[kind, pl.ds(0, TOK)] = jnp.where(lane < PAIR, query, 0.0).astype(BF16)
        q2[kind, pl.ds(TOK, TOK)] = jnp.where(lane >= PAIR, query, 0.0).astype(BF16)
        one, two = projected(1, kind)
        kvbuf[y, kind, c, :, pl.ds(HEAD, HEAD)] = two.astype(BF16)
        rec[2, kind] = one.astype(BF16)
        if kind == 0:
            kv_ring.begin(0)
            kv_ring.begin(1)
    for kind in range(2):
        one, two = projected(0, kind)
        rec[0, kind] = one.astype(BF16)
        rec[1, kind] = two.astype(BF16)
        if kind == 0:
            kv_ring.begin(2)
            kv_ring.begin(3)

    causal = lax.broadcasted_iota(jnp.int32, (BLOCK, BLOCK), 0) >= lax.broadcasted_iota(
        jnp.int32, (BLOCK, BLOCK), 1
    )
    tril = jnp.where(causal, 1.0, 0.0).astype(F32)
    gap = fg_ref[pl.ds(row, 1)]

    def segment(kind):
        shift = jnp.broadcast_to(dso[pl.ds(kind, 1)], (HEAD, TOK)).T
        state = jnp.zeros((HEAD, HEAD), F32)
        total = jnp.zeros((1, HEAD), F32)
        for b in range(TOK // BLOCK):
            rows = pl.ds(b * BLOCK, BLOCK)
            forget = rec[1, kind, rows].astype(F32)
            query = rec[0, kind, rows].astype(F32)
            value = rec[2, kind, rows]
            gate = gap * (1.0 / (1.0 + jnp.exp(forget)))
            decay = jnp.log1p(-gate) + shift[b * BLOCK : (b + 1) * BLOCK]
            cum = jnp.dot(tril, decay, precision=lax.Precision.HIGHEST, preferred_element_type=F32)
            end = cum[BLOCK - 1 :, :]
            q_dec = query * jnp.exp(cum)
            qdec[kind, rows] = (q_dec * jnp.exp(total)).astype(BF16)
            q_dec = q_dec.astype(BF16)
            k_grow = (gate * jnp.exp(-cum)).astype(BF16)
            scores = lax.dot_general(q_dec, k_grow, NT, preferred_element_type=F32)
            scores = jnp.where(causal, scores, 0.0).astype(BF16)
            out = jnp.dot(scores, value, preferred_element_type=F32)
            if b > 0:
                out = out + lax.dot_general(q_dec, state.astype(BF16), NT, preferred_element_type=F32)
            local[kind, rows] = out
            k_end = (gate * jnp.exp(end - cum)).astype(BF16)
            fresh = jnp.dot(value.astype(F32).T.astype(BF16), k_end, preferred_element_type=F32)
            state = state * jnp.exp(end) + fresh
            total = total + end
        pack(pair, (c, kind), state, total)

    def pack(buffer, where, state, total):
        buffer[(*where, pl.ds(0, HEAD))] = state.astype(BF16)
        high = total.astype(BF16)
        rest = total - high.astype(F32)
        middle = rest.astype(BF16)
        low = (rest - middle.astype(F32)).astype(BF16)
        index = lax.broadcasted_iota(jnp.int32, (ST_ROWS - HEAD, HEAD), 0)
        stack = jnp.where(
            index == 0, high.astype(F32), jnp.where(index == 1, middle.astype(F32), low.astype(F32))
        )
        buffer[(*where, pl.ds(HEAD, ST_ROWS - HEAD))] = stack.astype(BF16)

    def unpack(buffer, where):
        tail = buffer[(*where, pl.ds(HEAD, ST_ROWS - HEAD))].astype(F32)
        return buffer[(*where, pl.ds(0, HEAD))].astype(F32), tail[0:1] + tail[1:2] + tail[2:3]

    def pair_came(kind):
        ref = pair.at[1 - c, kind]
        remote(ref, ref, prs.at[kind], prr.at[kind], core).wait_recv()

    pair_sends = [
        remote(pair.at[c, kind], pair.at[c, kind], prs.at[kind], prr.at[kind], core) for kind in range(2)
    ]

    segment(0)
    pair_sends[0].start()
    segment(1)
    pair_sends[1].start()
    kv_ring.step(1, 0)
    kv_ring.step(1, 1)
    def keys_values(yo, kind):
        both = kvbuf[yo, kind].reshape(2 * TOK, 2 * HEAD)
        return both[:, :HEAD], both[:, HEAD:]

    kv_ring.wait_other(0)

    ones = jnp.ones((2 * TOK, HEAD), BF16)

    def own(kind, carry):
        keys, values = keys_values(y, kind)
        values = jnp.concatenate([values, ones], axis=1)
        halves_of = [pl.ds(part * TOK, TOK) for part in range(2)]
        queries = [q2[kind, rows] for rows in halves_of]
        seen = lax.broadcasted_iota(jnp.int32, (TOK, 2 * TOK), 1) <= (
            lax.broadcasted_iota(jnp.int32, (TOK, 2 * TOK), 0) + c * TOK
        )
        done = []
        for query in queries:
            scores = lax.dot_general(query, keys, NT, preferred_element_type=F32)
            scores = jnp.where(seen, scores, -jnp.inf)
            best = jnp.broadcast_to(jnp.max(scores, axis=-1, keepdims=True), (TOK, HEAD))
            expo = jnp.exp2((scores - jnp.concatenate([best] * 4, axis=1)) * SCORE_LOG2).astype(BF16)
            done.append((best, jnp.dot(expo, values, preferred_element_type=F32)))
        for rows, (best, total) in zip(halves_of, done):
            m_s[kind, rows] = best
            acc[kind, rows] = total
        return carry

    lax.fori_loop(0, 2, own, 0)
    kv_ring.step(1, 2)
    kv_ring.step(1, 3)
    pair_came(0)
    pair_came(1)
    early, early_total = unpack(pair, (0, c))
    late, late_total = unpack(pair, (1, c))
    pack(stbuf, (y, c), early * jnp.exp(late_total) + late, early_total + late_total)
    st_ring.begin(0)
    st_ring.begin(1)

    def absorb(yo, q_kind, kv_kind):
        keys, values = keys_values(yo, kv_kind)
        values = jnp.concatenate([values, ones], axis=1)
        halves_of = [pl.ds(part * TOK, TOK) for part in range(2)]
        queries = [q2[q_kind, rows] for rows in halves_of]
        olds = [m_s[q_kind, rows] for rows in halves_of]
        sums = [acc[q_kind, rows] for rows in halves_of]
        done = []
        for query, old, total in zip(queries, olds, sums):
            scores = lax.dot_general(query, keys, NT, preferred_element_type=F32)
            best = jnp.maximum(old, jnp.max(scores, axis=-1, keepdims=True))
            scale = jnp.exp2((old - best) * SCORE_LOG2)
            expo = jnp.exp2((scores - jnp.concatenate([best] * 4, axis=1)) * SCORE_LOG2).astype(BF16)
            fresh = jnp.dot(expo, values, preferred_element_type=F32)
            done.append((best, total * jnp.concatenate([scale] * 2, axis=1) + fresh))
        for rows, (best, total) in zip(halves_of, done):
            m_s[q_kind, rows] = best
            acc[q_kind, rows] = total

    def process(offset):
        if offset:
            kv_ring.wait_other(offset)
        yo = (y + offset + NY) % NY

        def unit(kind_at, carry):
            q_kind = jnp.where(kind_at == 0, 0, 1)
            kv_kind = jnp.where(kind_at == 2, 1, 0)
            wanted = jnp.where(kind_at == 1, linked.astype(jnp.int32), (yo < y).astype(jnp.int32))

            @pl.when(wanted == 1)
            def _():
                absorb(yo, q_kind, kv_kind)

            return carry

        lax.fori_loop(0, 3, unit, 0)

    process(0)
    for k in range(2, HALF + 1):
        kv_ring.step(k, 0)
        kv_ring.step(k, 1)
        process(1 - k)
        kv_ring.step(k, 2)
        kv_ring.step(k, 3)
        process(k - 1)
        st_ring.step(k - 1, 0)
        st_ring.step(k - 1, 1)
        if k == 2:
            wo_came(3, 1, 1)
            wo_on_right[1].start()
            wo_came(1, 3, 7)
            wo_on_left[1].start()
        elif k == 3:
            wo_came(3, 2, 2)
            wo_came(1, 0, 4)
        else:
            wo_came(3, 3, 3)
            wo_came(1, 1, 5)
            wo_came(2, 0, 8)
            wo_came(2, 2, 10)
    process(HALF)
    st_ring.step(HALF, 0)
    st_ring.step(HALF, 1)
    for offset in range(NY):
        st_ring.wait_other(offset)

    def pass_on(kind, yo, state):
        fresh, total = unpack(stbuf, (yo, kind))
        return state * jnp.exp(total) + fresh

    def within(kind, state):
        fresh, total = unpack(pair, (0, kind))
        after = state * jnp.exp(total) + fresh
        return jnp.where(c == 0, state, after)

    nothing = jnp.zeros((HEAD, HEAD), F32)
    into_low = lax.fori_loop(0, y, functools.partial(pass_on, 0), nothing)
    all_low = lax.fori_loop(y, NY, functools.partial(pass_on, 0), into_low)
    all_low = all_low * jnp.where(linked, 1.0, 0.0)
    into_high = lax.fori_loop(0, y, functools.partial(pass_on, 1), all_low)
    into_low, into_high = within(0, into_low), within(1, into_high)
    lam = lam_ref[row]
    token_parts = tuple(pl.ds(i * (TOK // 4), TOK // 4) for i in range(4))

    def mixed(kind):
        state = jnp.where(kind == 0, into_low, into_high).astype(BF16)
        raw = local[kind] + lax.dot_general(qdec[kind], state, NT, preferred_element_type=F32)
        mean_sq = jnp.mean(raw * raw, axis=-1, keepdims=True)
        rec_mix = (raw * lax.rsqrt(mean_sq + RECUR_EPSILON) * rgain_ref[...]).astype(BF16)
        low, high = acc[kind, pl.ds(0, TOK)], acc[kind, pl.ds(TOK, TOK)]
        raw = low[:, :HEAD] / low[:, HEAD:] - lam * (high[:, :HEAD] / high[:, HEAD:])
        mean_sq = jnp.mean(raw * raw, axis=-1, keepdims=True)
        att_mix = (raw * lax.rsqrt(mean_sq + ATTEND_EPSILON) * again_ref[...]).astype(BF16)
        return jnp.concatenate([rec_mix, att_mix], axis=1)

    def hop(group, head, i, slot, where):
        ref = gm.at[group, head, token_parts[i]]
        return remote(ref, ref, ms.at[slot], mr.at[slot], where)

    def came(group, head, i, slot):
        hop(group, head, i, slot, to_r).wait_recv()

    hops = []

    def go(*args):
        hops.append(hop(*args))
        hops[-1].start()

    give[...] = mixed(1 - row)
    gives = [
        remote(give.at[r], gm.at[x, row, r], ms.at[24 + i], mr.at[24 + i], {"sp_0": zp})
        for i, r in enumerate(token_parts)
    ]
    for i in (0, 2, 1, 3):
        gives[i].start()
    gm[x, row] = mixed(row)
    for i in range(4):
        go(x, row, i, i, to_r)
        go(x, row, (i + 2) % 4, 4 + (i + 2) % 4, to_l)

    def given(i):
        came(x, 1 - row, i, 24 + i)
        go(x, 1 - row, i, 12 + i, to_r)
        go(x, 1 - row, i, 16 + i, to_l)

    def relay(head, base, i):
        came(left, head, i, base + i)
        go(left, head, i, base + 8 + i, to_r)
        came(right, head, 2 + i, base + 6 + i)
        go(right, head, 2 + i, base + 10 + i, to_l)

    relay(row, 0, 0)
    given(0)
    relay(row, 0, 1)
    for i in (2, 1, 3):
        given(i)

    def product(group, j):
        parts = [gm[group, h, :, pl.ds(p * HEAD, HEAD)] for p in range(2) for h in range(2)]
        weight = wobuf[group, j // 2, :, pl.ds((j % 2) * width, width)]
        out = jnp.dot(jnp.concatenate(parts, axis=1), weight, preferred_element_type=F32)
        return out.astype(BF16).astype(F32)

    def wo_ready(offset):
        for i in range(4):
            ref = wobuf.at[(x + offset) % NX, 1 - c, pl.ds(i * HEAD, HEAD)]
            n = 4 * (offset - 1) + i
            remote(ref, ref, wops.at[n], wopr.at[n], core).wait_recv()

    width = OUT_HALF // 2
    for j in range(4):
        sums[:, pl.ds(j * width, width)] = product(x, j)
    relay(1 - row, 12, 0)
    relay(1 - row, 12, 1)
    wo_came(2, 1, 9)
    wo_came(2, 3, 11)
    for offset in (1, 2, 3):
        wo_ready(offset)
    for i in range(2):
        for base, head in ((0, row), (12, 1 - row)):
            came(left, head, 2 + i, base + 2 + i)
            came(right, head, i, base + 4 + i)

    def near(i, carry):
        group = jnp.where(i == 0, left, right)
        for j in range(4):
            cols = pl.ds(j * width, width)
            sums[:, cols] = sums[:, cols] + product(group, j)
        return carry

    lax.fori_loop(0, 2, near, 0)
    for i in range(4):
        came(far, row, i, 8 + i)
        came(far, 1 - row, i, 20 + i)
    puts = []
    for j in range(4):
        cols = pl.ds(j * width, width)
        out_ref[:, cols] = (sums[:, cols] + product(far, j)).astype(BF16)
        puts.append(pltpu.make_async_copy(out_ref.at[:, cols], res_ref.at[:, cols], put.at[j]))
        puts[-1].start()
    w_ring.finish()
    kv_ring.finish()
    st_ring.finish()
    sent = list(spread.values()) + across + [shifts] + t2_right + t2_left + t2_on_right + t2_on_left
    sent += wo_right + wo_left + wo_on_right + wo_on_left + list(wo_push.values()) + gives + hops + pair_sends
    for copy in sent:
        copy.wait_send()
    for copy in puts:
        copy.wait()


def per_device(
    tokens_in, norm_gain, rec_query_weight, rec_forget_weight, rec_input_weight, att_query_weight,
    att_key_weight, att_value_weight, recurrence_output_weight, out_att_weight, floor_gap,
    decay_shift, rec_gain, att_gain, lambda_head,
):
    width = PAIR // 2
    steps = np.arange(width, dtype=np.float32) / np.float32(width)
    frequency = np.float32(1.0) / np.float32(ROTARY_BASE) ** steps
    frequency = np.concatenate([frequency] * 4)[None].astype(np.float32)
    d_model = tokens_in.shape[1]
    return pl.pallas_call(
        layer_kernel,
        name="layer",
        out_shape=jax.ShapeDtypeStruct((TOK, d_model), BF16),
        in_specs=[HBM] * 15 + [pl.BlockSpec(memory_space=pltpu.SMEM)],
        out_specs=HBM,
        scratch_shapes=[
            pltpu.VMEM((TOK, d_model), BF16),
            pltpu.VMEM((2, TOK), F32),
            pltpu.VMEM((1, d_model), F32),
            pltpu.VMEM((1, HEAD), F32),
            pltpu.VMEM((2, HEAD), F32),
            pltpu.VMEM((1, HEAD), F32),
            pltpu.VMEM((1, HEAD), F32),
            pltpu.VMEM((NX, QUART, d_model), BF16),
            pltpu.VMEM((NX, QUART, d_model), BF16),
            pltpu.VMEM((2, TOK, d_model), BF16),
            pltpu.VMEM((16, 6 * HEAD), BF16),
            pltpu.VMEM((NZ, NY, 2, 16, 6 * HEAD), BF16),
            pltpu.VMEM((2, TOK), F32),
            pltpu.VMEM((2, TOK), F32),
            pltpu.VMEM((NX, 2, 4 * HEAD, OUT_HALF), BF16),
            pltpu.VMEM((3, 2, TOK, HEAD), BF16),
            pltpu.VMEM((NY, 2, 2, TOK, 2 * HEAD), BF16),
            pltpu.VMEM((NY, 2, ST_ROWS, HEAD), BF16),
            pltpu.VMEM((2, 2, ST_ROWS, HEAD), BF16),
            pltpu.VMEM((2, 2 * TOK, HEAD), BF16),
            pltpu.VMEM((2, 2 * TOK, HEAD), F32),
            pltpu.VMEM((2, TOK, HEAD), F32),
            pltpu.VMEM((2, 2 * TOK, 2 * HEAD), F32),
            pltpu.VMEM((2, TOK, HEAD), F32),
            pltpu.VMEM((2, TOK, HEAD), BF16),
            pltpu.VMEM((TOK, 2 * HEAD), BF16),
            pltpu.VMEM((NX, 2, TOK, 2 * HEAD), BF16),
            pltpu.VMEM((TOK, d_model), F32),
            DMA((26,)),
            DMA((4,)), DMA((4,)), DMA((12,)), DMA((12,)), DMA((1,)), DMA((1,)),
            DMA((NZ - 1,)), DMA((NZ - 1,)), DMA((12,)), DMA((12,)), DMA((12,)), DMA((12,)),
            DMA((28,)), DMA((28,)), DMA((4,)), DMA((2,)), DMA((2,)),
            *ring_sems(4), *ring_sems(4), *ring_sems(2),
        ],
        compiler_params=pltpu.CompilerParams(
            collective_id=0, has_side_effects=True, vmem_limit_bytes=VMEM_LIMIT
        ),
    )(
        tokens_in.reshape(NX, QUART, d_model), rec_query_weight, rec_forget_weight, rec_input_weight,
        att_value_weight, att_query_weight, att_key_weight, recurrence_output_weight, out_att_weight,
        decay_shift, norm_gain[None], jnp.asarray(frequency), floor_gap.reshape(2, HEAD),
        rec_gain[None], att_gain[None], lambda_head,
    )


def solution(mesh):
    split = Mesh(mesh.devices.reshape(NZ, NY, 2, NX), ("sp_0", "sp_1", "sp_2", "tp"))
    placed = (
        P(SP, None), P(), P(SP, "tp"), P(SP, "tp"), P(SP, "tp"), P(SP, "tp"), P(SP, "tp"), P(SP, "tp"),
        P("tp", None), P("tp", None), P("tp"), P("tp", SP), P(), P(), P("tp"),
    )
    return jax.shard_map(
        per_device, mesh=split, in_specs=placed, out_specs=P(SP, None), check_vma=False
    )
```
